32 devices in a mesh: fs: 8 (over z, core), tp: 4 (over y, x).
Axes of the slice: x: 2, y: 2, z: 4, core: 2. Of those that a mesh axis runs over, the one named last changes fastest.
Arguments:
- prompt: bfloat16 [1024, 2048], P('tp'), may hold values from -6 to 6
- norm_gain: float32 [2048], P('fs'), may hold values from 0.1 to 1.9
- gate_master: float32 [32, 2048, 512], P(None, 'fs', 'tp'), may hold values from -6 to 6
- up_master: float32 [32, 2048, 512], P(None, 'fs', 'tp'), may hold values from -6 to 6
- down_master: float32 [32, 2048, 512], P(None, 'fs', 'tp'), may hold values from -6 to 6
- group_choice: int32 [1024], P('tp'), may hold values from 0 to 3
- inner_choice: int32 [1024, 2], P('tp'), may hold values from 0 to 7, as said below
- route_weight: float32 [1024, 2], P('tp'), may hold values from 0.2 to 1
Outputs:
- gate_served: bfloat16 [2048, 16384], P(None, 'fs')
- up_served: bfloat16 [2048, 16384], P(None, 'fs')
- down_served: bfloat16 [2048, 16384], P(None, 'fs')
- mixed: bfloat16 [1024, 2048], P('tp', 'fs')
The draws below stay inside these ranges and needn't reach their ends.
Inputs may be any that keep to these rules, and one draw needn't show every extreme that they name: `inner_choice`: the two experts of a token differ.
All inputs are finite; a program needn't handle non-finite values.
Results may differ from the reference program's by a relative error of at most 0.0081.
Values may be sent and summed in bfloat16 or wider, within the bound.
A program may use at most 128 MiB of HBM per device.

```python
import math
import jax
import jax.numpy as jnp
from jax import lax

D = 2048
FF = 512
GROUPS = 4
EPG = 8
TOK_DEV = 256
EXPERTS = 32
TOKENS = 1024


def routing_draw(key):
    base = jax.random.fold_in(key, 7411)
    keys = jax.random.split(base, 9)
    shards = TOKENS // TOK_DEV
    hot_group = jax.random.randint(keys[0], (shards,), 0, GROUPS)
    hot_inner = jax.random.randint(keys[1], (shards,), 0, EPG)
    hot_count = jax.random.randint(keys[2], (shards,), 0, TOK_DEV // 2 + 1)
    heavy = jax.random.randint(keys[3], (), 0, shards)
    hot_count = jnp.where(jnp.arange(shards) == heavy, 3 * TOK_DEV // 4, hot_count)
    ranks = jax.vmap(lambda sub: jax.random.permutation(sub, TOK_DEV))(jax.random.split(keys[4], shards))
    hot = (ranks < hot_count[:, None]).reshape(TOKENS)
    shard_of = jnp.arange(TOKENS) // TOK_DEV
    drawn_group = jax.random.randint(keys[5], (TOKENS,), 0, GROUPS)
    first_drawn = jax.random.randint(keys[6], (TOKENS,), 0, EPG)
    offsets = jax.random.randint(keys[7], (TOKENS,), 1, EPG)
    flip = jax.random.randint(keys[8], (TOKENS,), 0, 2)
    group = jnp.where(hot, hot_group[shard_of], drawn_group)
    first = jnp.where(hot, hot_inner[shard_of], first_drawn)
    second = (first + offsets) % EPG
    pair = jnp.where(flip[:, None] == 1, jnp.stack([second, first], axis=1), jnp.stack([first, second], axis=1))
    return (group.astype(jnp.int32), pair.astype(jnp.int32))


def draw_group_choice(key, part):
    group, pair = routing_draw(key)
    return group


def draw_inner_choice(key, part):
    group, pair = routing_draw(key)
    return pair


def levels(key, shape, cuts, smallest, high):
    def one(dim, blocks):
        steps = jax.random.uniform(jax.random.fold_in(jax.random.fold_in(key, 6), dim), (blocks,), jnp.float32, smallest / len(cuts), high / len(cuts))
        return jnp.repeat(jnp.exp(steps), shape[dim] // blocks).reshape((-1,) + (1,) * (len(shape) - dim - 1))

    loudness = one(*cuts[0])
    for cut in cuts[1:]:
        loudness = loudness * one(*cut)
    return loudness


def scatter_about(rng, extent, scale, reach, pieces=(), kind=jnp.bfloat16):
    drawn = jax.random.normal(rng, extent, jnp.float32) * scale
    if len(pieces) > 0:
        drawn = levels(rng, extent, pieces, -0.22, 0.18) * drawn
    return jnp.clip(drawn, min=-reach, max=reach).astype(kind)


def setup_inputs(seed: int = 0) -> dict:
    seeds = jax.random.split(jax.random.key(seed), 9)
    prompt = scatter_about(seeds[0], (TOKENS, D), 1.0, 6.0, ((0, 4),))
    norm_gain = jnp.clip(1.0 + 0.18 * jax.random.normal(seeds[1], (D,), jnp.float32), 0.1, 1.9)
    gate_master = scatter_about(seeds[2], (EXPERTS, D, FF), 1.0, 6.0, ((1, 8), (2, 4)), jnp.float32)
    up_master = scatter_about(seeds[3], (EXPERTS, D, FF), 1.0, 6.0, ((1, 8), (2, 4)), jnp.float32)
    down_master = scatter_about(seeds[4], (EXPERTS, D, FF), 1.0, 6.0, ((1, 8), (2, 4)), jnp.float32)
    group_choice = draw_group_choice(jax.random.fold_in(seeds[8], 71), 0)
    inner_choice = draw_inner_choice(jax.random.fold_in(seeds[8], 71), 0)
    route_weight = jnp.clip(jnp.exp(math.log(1.0) - 1.609438 * jax.random.uniform(seeds[7], (TOKENS, 2), jnp.float32) ** levels(seeds[7], (TOKENS, 2), ((0, 4),), -0.2, 0.2)), 0.2, 1.0)
    return dict(prompt=prompt, norm_gain=norm_gain, gate_master=gate_master, up_master=up_master, down_master=down_master, group_choice=group_choice, inner_choice=inner_choice, route_weight=route_weight)


def reference(prompt, norm_gain, gate_master, up_master, down_master, group_choice, inner_choice, route_weight):
    experts = GROUPS * EPG
    scale = norm_gain[None, :, None]
    gate_served = (gate_master * scale).astype(jnp.bfloat16).transpose(1, 0, 2).reshape(D, experts * FF)
    up_served = (up_master * scale).astype(jnp.bfloat16).transpose(1, 0, 2).reshape(D, experts * FF)
    down_served = down_master.astype(jnp.bfloat16).transpose(1, 0, 2).reshape(D, experts * FF)
    values = prompt.astype(jnp.float32)
    normed = (values * lax.rsqrt(lax.optimization_barrier(jnp.mean(values * values, axis=1, keepdims=True)) + 1e-06)).astype(jnp.bfloat16)
    chosen = group_choice[:, None] * EPG + inner_choice
    member = (chosen[:, :, None] == jnp.arange(experts, dtype=jnp.int32)[None, None, :]).astype(jnp.float32)
    weight = lax.optimization_barrier(jnp.sum(member * route_weight[:, :, None], axis=1))

    def one_expert(total, index):
        begin = (index * FF).astype(jnp.int32)
        gate_cols = lax.dynamic_slice_in_dim(gate_served, begin, FF, 1)
        up_cols = lax.dynamic_slice_in_dim(up_served, begin, FF, 1)
        down_cols = lax.dynamic_slice_in_dim(down_served, begin, FF, 1)
        gate_act = jnp.dot(normed, gate_cols, preferred_element_type=jnp.float32) * D ** (-0.5)
        up_act = jnp.dot(normed, up_cols, preferred_element_type=jnp.float32) * D ** (-0.5)
        column = lax.dynamic_slice_in_dim(weight, index.astype(jnp.int32), 1, 1)
        scaled = (column * jax.nn.silu(gate_act) * up_act).astype(jnp.bfloat16)
        part = lax.dot_general(scaled, down_cols, (((1,), (1,)), ((), ())), preferred_element_type=jnp.float32)
        return (total + part, None)
    total, _ = lax.scan(one_expert, jnp.zeros((prompt.shape[0], D), jnp.float32), jnp.arange(experts, dtype=jnp.int32))
    mixed = (total * FF ** (-0.5)).astype(jnp.bfloat16)
    return (gate_served, up_served, down_served, mixed)
```

```python
import jax
import jax.numpy as jnp
from jax import lax
from jax.experimental import pallas as pl
from jax.experimental.pallas import tpu as pltpu
from jax.sharding import PartitionSpec as P

MESH = pl.DeviceIdType.MESH
FF = 512
GROUPS = 4
EPG = 8


def flatten_rows(piece):
    count, experts, rows, hidden = piece.shape
    return piece.transpose(0, 2, 1, 3).reshape(count, rows, experts * hidden)


def restore_rows(gathered, rows):
    parts = lax.axis_size("tp")
    count, total, width = gathered.shape
    blocks = total // (parts * rows)
    ordered = gathered.reshape(count, parts, blocks, rows, width).transpose(0, 2, 1, 3, 4)
    return ordered.reshape(count, total, width)


def activations(normed, gate_local, up_local, column_weight):
    width = normed.shape[1]
    gate_act = jnp.dot(normed, gate_local, preferred_element_type=jnp.float32) * width ** (-0.5)
    up_act = jnp.dot(normed, up_local, preferred_element_type=jnp.float32) * width ** (-0.5)
    return (column_weight * jax.nn.silu(gate_act) * up_act).astype(jnp.bfloat16)


def route_columns(weight, columns, experts):
    first = lax.axis_index("fs") * columns
    owner = (first + jnp.arange(columns, dtype=jnp.int32)) // FF
    onehot = (owner[None, :] == jnp.arange(experts, dtype=jnp.int32)[:, None]).astype(jnp.float32)
    return jnp.dot(weight, onehot, precision=lax.Precision.HIGHEST)


def shards(
    prompt, norm_gain, gate_master, up_master, down_master, group_choice, inner_choice, route_weight
):
    experts = GROUPS * EPG
    scale = norm_gain[None, :, None]
    gate_cast = (gate_master * scale).astype(jnp.bfloat16)
    up_cast = (up_master * scale).astype(jnp.bfloat16)
    down_cast = down_master.astype(jnp.bfloat16)
    rows = gate_master.shape[1] // lax.axis_size("tp")
    values = prompt.astype(jnp.float32)
    normed = (values * lax.rsqrt(jnp.mean(values * values, axis=1, keepdims=True) + 1e-06)).astype(
        jnp.bfloat16
    )
    chosen = group_choice[:, None] * EPG + inner_choice
    member = (chosen[:, :, None] == jnp.arange(experts, dtype=jnp.int32)[None, None, :]).astype(
        jnp.float32
    )
    weight = jnp.sum(member * route_weight[:, :, None], axis=1)
    stacked = jnp.stack([gate_cast, up_cast, down_cast])
    widened = lax.all_to_all(stacked, "tp", split_axis=2, concat_axis=3, tiled=True)
    moved = lax.all_to_all(flatten_rows(widened), "fs", split_axis=2, concat_axis=1, tiled=True)
    served = restore_rows(lax.all_gather(moved, "tp", axis=1, tiled=True), rows)
    gate_local, up_local, down_local = (served[0], served[1], served[2])
    column_weight = route_columns(weight, gate_local.shape[1], experts)
    scaled = activations(normed, gate_local, up_local, column_weight)
    summed = lax.psum_scatter(
        lax.dot_general(
            down_local, scaled, (((1,), (1,)), ((), ())), preferred_element_type=jnp.float32
        ),
        "fs",
        scatter_dimension=0,
        tiled=True,
    )
    mixed = (summed * FF ** (-0.5)).T.astype(jnp.bfloat16)
    return (gate_local, up_local, down_local, mixed)


def spread_body(
    gain_ref,
    gate_ref,
    up_ref,
    down_ref,
    prompt_ref,
    group_ref,
    inner_ref,
    route_ref,
    served,
    scaled,
    got,
    raw,
    cast,
    gain,
    scale,
    prompt,
    normed,
    group,
    inner,
    route,
    column,
    part,
    load_sem,
    small_sem,
    zs,
    zr,
    xs,
    xr,
    ys,
    yr,
    fxs,
    fxr,
    fys,
    fyr,
    ps,
    pr,
):
    f, t = lax.axis_index("fs"), lax.axis_index("tp")
    tx, ty, td = jnp.bitwise_xor(t, 1), jnp.bitwise_xor(t, 2), jnp.bitwise_xor(t, 3)
    arrays, groups, per, rows, hidden = raw.shape
    parts, tokens = served.shape[1], prompt.shape[0]
    half = rows // 2
    masters = (gate_ref, up_ref, down_ref)

    def peer(k):
        return jnp.bitwise_xor(f, k)

    def load(w, k):
        return pltpu.make_async_copy(masters[w].at[peer(k)], raw.at[w, k], load_sem.at[w, k])

    small = [
        pltpu.make_async_copy(source, target, small_sem.at[i])
        for i, (source, target) in enumerate(
            (
                (gain_ref, gain),
                (prompt_ref, prompt),
                (group_ref, group),
                (inner_ref, inner),
                (route_ref, route),
            )
        )
    ]

    def block(w, origin, k, begin=0, count=rows):
        first = pl.multiple_of(peer(k) * rows + begin, count)
        return served.at[w, origin, pl.ds(first, count)]

    def z_copy(w, k):
        return pltpu.make_async_remote_copy(
            src_ref=cast.at[w, k - 1],
            dst_ref=block(w, t, 0),
            send_sem=zs.at[w, k],
            recv_sem=zr.at[w, k],
            device_id={"fs": peer(k), "tp": t},
            device_id_type=MESH,
        )

    def z_arrival(w, k):
        return pltpu.make_async_remote_copy(
            src_ref=cast.at[w, k - 1],
            dst_ref=block(w, t, k),
            send_sem=zs.at[w, k],
            recv_sem=zr.at[w, k],
            device_id={"fs": peer(k), "tp": t},
            device_id_type=MESH,
        )

    def side_copy(w, k, origin, target, send, recv):
        return pltpu.make_async_remote_copy(
            src_ref=block(w, origin, k),
            dst_ref=block(w, origin, k),
            send_sem=send.at[w, k],
            recv_sem=recv.at[w, k],
            device_id={"fs": f, "tp": target},
            device_id_type=MESH,
        )

    def half_copy(w, k, origin, which, target, send, recv):
        piece = block(w, origin, k, which * half, half)
        return pltpu.make_async_remote_copy(
            src_ref=piece,
            dst_ref=piece,
            send_sem=send.at[w, k],
            recv_sem=recv.at[w, k],
            device_id={"fs": f, "tp": target},
            device_id_type=MESH,
        )

    def part_copy(k):
        return pltpu.make_async_remote_copy(
            src_ref=part.at[k - 1],
            dst_ref=got.at[k - 1],
            send_sem=ps.at[k],
            recv_sem=pr.at[k],
            device_id={"fs": peer(k), "tp": t},
            device_id_type=MESH,
        )

    def side_start(w, k):
        side_copy(w, k, t, tx, xs, xr).start()
        side_copy(w, k, t, ty, ys, yr).start()

    def forward(w, k):
        side_copy(w, k, tx, tx, xs, xr).wait_recv()
        half_copy(w, k, tx, 0, ty, fys, fyr).start()
        side_copy(w, k, ty, ty, ys, yr).wait_recv()
        half_copy(w, k, ty, 1, tx, fxs, fxr).start()

    def diagonal_wait(w, k):
        half_copy(w, k, td, 0, ty, fys, fyr).wait_recv()
        half_copy(w, k, td, 1, tx, fxs, fxr).wait_recv()

    def put(w, k, target):
        load(w, k).wait()
        for e in range(per):
            value = raw[w, k, e]
            if w < 2:
                value = value * scale[...]
            target[:, e * hidden : (e + 1) * hidden] = value.astype(jnp.bfloat16)

    def put_own(w):
        put(w, 0, block(w, t, 0))

    def put_away(w, k):
        put(w, k, cast.at[w, k - 1])

    def normalise():
        small[1].wait()
        values = prompt[...].astype(jnp.float32)
        mean = jnp.mean(values * values, axis=1, keepdims=True)
        normed[...] = (values * lax.rsqrt(mean + 1e-06)).astype(jnp.bfloat16)

    def columns():
        for i in range(2, 5):
            small[i].wait()
        chosen = group[...] * EPG + inner[...]
        for e in range(per):
            weight = jnp.sum(jnp.where(chosen == f * per + e, route[...], 0.0), axis=0, keepdims=True)
            column[:, e * hidden : (e + 1) * hidden] = jnp.broadcast_to(weight, (hidden, tokens)).T

    def hidden_units(origin):
        step = 2 * hidden
        for n in range(per // 2):
            at = pl.ds(n * step, step)
            scaled[origin, :, at] = activations(
                normed[...], served[0, origin, :, at], served[1, origin, :, at], column[:, at]
            )

    def features(k):
        total = None
        for i in range(parts):
            term = lax.dot_general(
                scaled[i],
                block(2, i, k)[...],
                (((1,), (1,)), ((), ())),
                preferred_element_type=jnp.float32,
            )
            total = term if total is None else total + term
        part[k - 1] = total.astype(jnp.bfloat16)

    last = list(range(groups - 1, -1, -1))
    order = [(w, k) for w in range(2) for k in range(groups)] + [(2, k) for k in last]
    away = [list(range(1, groups)), list(range(1, groups)), last[:-1]]

    small[0].start()
    load(0, 0).start()
    barrier = pltpu.get_barrier_semaphore()
    for k in range(1, groups):
        pl.semaphore_signal(barrier, inc=1, device_id={"fs": peer(k), "tp": t}, device_id_type=MESH)
    for other in (tx, ty):
        pl.semaphore_signal(barrier, inc=1, device_id={"fs": f, "tp": other}, device_id_type=MESH)
    for k in away[0]:
        load(0, k).start()
    for w in (1, 2):
        load(w, 0).start()
        for k in away[w]:
            load(w, k).start()
    for copy in small[1:]:
        copy.start()
    small[0].wait()
    scale[...] = jnp.broadcast_to(gain[...], (hidden, rows)).T
    put_own(0)
    put_away(0, 1)
    pl.semaphore_wait(barrier, groups + 1)
    side_start(0, 0)

    def first_away(k, carry):
        put_away(0, k)
        z_copy(0, k - 1).start()
        return carry

    lax.fori_loop(2, groups, first_away, 0)
    z_copy(0, groups - 1).start()

    def later_away(w):
        def one(k, carry):
            put_away(w, k)
            return carry

        put_own(w)
        lax.fori_loop(1, groups, one, 0)

    base = 2 * groups
    for s, (w, k) in enumerate(order):
        if s > 0:
            if k > 0:
                z_arrival(w, k).wait_recv()
            side_start(w, k)
            forward(*order[s - 1])
        if s == 0:
            later_away(1)
        if s == 1:
            later_away(2)
        if w < 2 and k > 0:
            z_copy(w + 1, away[w + 1][k - 1]).start()
        if s == groups:
            normalise()
            columns()
        if s == base:
            hidden_units(t)
        if s == base + 1:
            hidden_units(tx)
            hidden_units(ty)
        if s == base + 2:
            for i in range(base):
                diagonal_wait(*order[i])
            hidden_units(td)
        if s >= base + 2:
            one = order[s - 2][1]
            diagonal_wait(2, one)
            features(one)
            part_copy(one).start()
    forward(*order[-1])
    diagonal_wait(2, 1)
    features(1)
    part_copy(1).start()
    diagonal_wait(2, 0)

    def finish(w, carry):
        def one(k, inner):
            side_copy(w, k, t, tx, xs, xr).wait_send()
            side_copy(w, k, t, ty, ys, yr).wait_send()
            half_copy(w, k, tx, 0, ty, fys, fyr).wait_send()
            half_copy(w, k, ty, 1, tx, fxs, fxr).wait_send()
            return inner

        def two(k, inner):
            z_copy(w, k).wait_send()
            return inner

        lax.fori_loop(0, groups, one, 0)
        lax.fori_loop(1, groups, two, 0)
        return carry

    lax.fori_loop(0, arrays, finish, 0)
    for k in range(1, groups):
        part_copy(k).wait_recv()
        part_copy(k).wait_send()


def spread(prompt, norm_gain, gate_master, up_master, down_master, group_choice, inner_choice, route_weight):
    groups, parts = lax.axis_size("fs"), lax.axis_size("tp")
    experts, rows, hidden = gate_master.shape
    per = experts // groups
    tokens, width = prompt.shape
    arrays = 3
    views = [one.reshape(groups, per, rows, hidden) for one in (gate_master, up_master, down_master)]
    dma = pltpu.SemaphoreType.DMA
    return pl.pallas_call(
        spread_body,
        in_specs=[pl.BlockSpec(memory_space=pltpu.HBM)] * 8,
        out_specs=[pl.BlockSpec(memory_space=pltpu.VMEM)] * 3,
        out_shape=[
            pltpu.VMEM((arrays, parts, width, per * hidden), jnp.bfloat16),
            pltpu.VMEM((parts, tokens, per * hidden), jnp.bfloat16),
            pltpu.VMEM((groups - 1, tokens, rows), jnp.bfloat16),
        ],
        scratch_shapes=[
            pltpu.VMEM((arrays, groups, per, rows, hidden), jnp.float32),
            pltpu.VMEM((arrays, groups - 1, rows, per * hidden), jnp.bfloat16),
            pltpu.VMEM((1, rows), jnp.float32),
            pltpu.VMEM((rows, hidden), jnp.float32),
            pltpu.VMEM((tokens, width), jnp.bfloat16),
            pltpu.VMEM((tokens, width), jnp.bfloat16),
            pltpu.VMEM((1, tokens), jnp.int32),
            pltpu.VMEM((2, tokens), jnp.int32),
            pltpu.VMEM((2, tokens), jnp.float32),
            pltpu.VMEM((tokens, per * hidden), jnp.float32),
            pltpu.VMEM((groups - 1, tokens, rows), jnp.bfloat16),
            dma((arrays, groups)),
            dma((5,)),
        ]
        + [dma((arrays, groups))] * 10
        + [dma((groups,))] * 2,
        compiler_params=pltpu.CompilerParams(
            collective_id=0, has_side_effects=True, vmem_limit_bytes=32 * 1024 * 1024
        ),
        name="spread",
    )(
        norm_gain.reshape(1, rows),
        *views,
        prompt,
        group_choice.reshape(1, tokens),
        inner_choice.T,
        route_weight.T,
    )


def serve_body(served, scaled, got, gate_ref, up_ref, down_ref, mixed_ref, sem):
    arrays, parts, _, wide = served.shape
    rows = got.shape[2]
    hidden = FF // parts
    f = lax.axis_index("fs")
    copies = []
    for w, out in enumerate((gate_ref, up_ref, down_ref)):
        for i in range(parts):
            for e in range(wide // hidden):
                copies.append(
                    pltpu.make_async_copy(
                        served.at[w, i, :, pl.ds(e * hidden, hidden)],
                        out.at[:, pl.ds(e * FF + i * hidden, hidden)],
                        sem.at[len(copies)],
                    )
                )
    for copy in copies:
        copy.start()
    total = None
    for i in range(parts):
        term = lax.dot_general(
            scaled[i],
            served[2, i, pl.ds(pl.multiple_of(f * rows, rows), rows), :],
            (((1,), (1,)), ((), ())),
            preferred_element_type=jnp.float32,
        )
        total = term if total is None else total + term
    for k in range(got.shape[0]):
        total = total + got[k].astype(jnp.float32)
    mixed_ref[...] = (total * FF ** (-0.5)).astype(jnp.bfloat16)
    for copy in copies:
        copy.wait()


def serve(served, scaled, got):
    arrays, parts, width, wide = served.shape
    _, tokens, rows = got.shape
    out = jax.ShapeDtypeStruct((width, parts * wide), served.dtype)
    vmem, hbm = pl.BlockSpec(memory_space=pltpu.VMEM), pl.BlockSpec(memory_space=pltpu.HBM)
    return pl.pallas_call(
        serve_body,
        in_specs=[vmem, vmem, vmem],
        out_specs=[hbm, hbm, hbm, vmem],
        out_shape=[out, out, out, jax.ShapeDtypeStruct((tokens, rows), jnp.bfloat16)],
        scratch_shapes=[pltpu.SemaphoreType.DMA((arrays * parts * (parts * wide // FF),))],
        compiler_params=pltpu.CompilerParams(vmem_limit_bytes=4 * 1024 * 1024),
        name="serve",
    )(*[pltpu.with_memory_space_constraint(one, pltpu.VMEM) for one in (served, scaled, got)])


def direct_shards(
    prompt, norm_gain, gate_master, up_master, down_master, group_choice, inner_choice, route_weight
):
    served, scaled, got = spread(
        prompt, norm_gain, gate_master, up_master, down_master, group_choice, inner_choice, route_weight
    )
    return tuple(serve(served, scaled, got))


def fits_direct(mesh):
    groups, parts = mesh.shape["fs"], mesh.shape["tp"]
    whole_experts = (GROUPS * EPG) % groups == 0 and (GROUPS * EPG // groups) % 2 == 0
    return parts == 4 and groups >= 4 and groups & (groups - 1) == 0 and whole_experts and FF // parts % 128 == 0


def solution(mesh):
    in_specs = (
        P("tp", None),
        P("fs"),
        P(None, "fs", "tp"),
        P(None, "fs", "tp"),
        P(None, "fs", "tp"),
        P("tp"),
        P("tp", None),
        P("tp", None),
    )
    out_specs = (P(None, "fs"), P(None, "fs"), P(None, "fs"), P("tp", "fs"))
    body = direct_shards if fits_direct(mesh) else shards
    return jax.shard_map(body, mesh=mesh, in_specs=in_specs, out_specs=out_specs, check_vma=False)
```

```python
import jax
import jax.numpy as jnp
from jax import lax
from jax.experimental import pallas as pl
from jax.experimental.pallas import tpu as pltpu
from jax.sharding import PartitionSpec as P

MESH = pl.DeviceIdType.MESH
FF = 512
GROUPS = 4
EPG = 8


def flatten_rows(piece):
    count, experts, rows, hidden = piece.shape
    return piece.transpose(0, 2, 1, 3).reshape(count, rows, experts * hidden)


def restore_rows(gathered, rows):
    parts = lax.axis_size("tp")
    count, total, width = gathered.shape
    blocks = total // (parts * rows)
    ordered = gathered.reshape(count, parts, blocks, rows, width).transpose(0, 2, 1, 3, 4)
    return ordered.reshape(count, total, width)


def activations(normed, gate_local, up_local, column_weight):
    width = normed.shape[1]
    gate_act = jnp.dot(normed, gate_local, preferred_element_type=jnp.float32) * width ** (-0.5)
    up_act = jnp.dot(normed, up_local, preferred_element_type=jnp.float32) * width ** (-0.5)
    return (column_weight * jax.nn.silu(gate_act) * up_act).astype(jnp.bfloat16)


def route_columns(weight, columns, experts):
    first = lax.axis_index("fs") * columns
    owner = (first + jnp.arange(columns, dtype=jnp.int32)) // FF
    onehot = (owner[None, :] == jnp.arange(experts, dtype=jnp.int32)[:, None]).astype(jnp.float32)
    return jnp.dot(weight, onehot, precision=lax.Precision.HIGHEST)


def shards(
    prompt, norm_gain, gate_master, up_master, down_master, group_choice, inner_choice, route_weight
):
    experts = GROUPS * EPG
    scale = norm_gain[None, :, None]
    gate_cast = (gate_master * scale).astype(jnp.bfloat16)
    up_cast = (up_master * scale).astype(jnp.bfloat16)
    down_cast = down_master.astype(jnp.bfloat16)
    rows = gate_master.shape[1] // lax.axis_size("tp")
    values = prompt.astype(jnp.float32)
    normed = (values * lax.rsqrt(jnp.mean(values * values, axis=1, keepdims=True) + 1e-06)).astype(
        jnp.bfloat16
    )
    chosen = group_choice[:, None] * EPG + inner_choice
    member = (chosen[:, :, None] == jnp.arange(experts, dtype=jnp.int32)[None, None, :]).astype(
        jnp.float32
    )
    weight = jnp.sum(member * route_weight[:, :, None], axis=1)
    stacked = jnp.stack([gate_cast, up_cast, down_cast])
    widened = lax.all_to_all(stacked, "tp", split_axis=2, concat_axis=3, tiled=True)
    moved = lax.all_to_all(flatten_rows(widened), "fs", split_axis=2, concat_axis=1, tiled=True)
    served = restore_rows(lax.all_gather(moved, "tp", axis=1, tiled=True), rows)
    gate_local, up_local, down_local = (served[0], served[1], served[2])
    column_weight = route_columns(weight, gate_local.shape[1], experts)
    scaled = activations(normed, gate_local, up_local, column_weight)
    summed = lax.psum_scatter(
        lax.dot_general(
            down_local, scaled, (((1,), (1,)), ((), ())), preferred_element_type=jnp.float32
        ),
        "fs",
        scatter_dimension=0,
        tiled=True,
    )
    mixed = (summed * FF ** (-0.5)).T.astype(jnp.bfloat16)
    return (gate_local, up_local, down_local, mixed)


def spread_body(
    gain_ref,
    gate_ref,
    up_ref,
    down_ref,
    prompt_ref,
    group_ref,
    inner_ref,
    route_ref,
    served,
    scaled,
    got,
    raw,
    cast,
    gain,
    scale,
    prompt,
    normed,
    group,
    inner,
    route,
    column,
    part,
    load_sem,
    bulk_sem,
    small_sem,
    send_sem,
    zr,
    xr,
    yr,
    dr,
    pr,
):
    f, t = lax.axis_index("fs"), lax.axis_index("tp")
    tx, ty, td = jnp.bitwise_xor(t, 1), jnp.bitwise_xor(t, 2), jnp.bitwise_xor(t, 3)
    arrays, groups, per, rows, hidden = raw.shape
    parts, width = served.shape[1:3]
    tokens = prompt.shape[0]
    half = rows // 2
    masters = (gate_ref, up_ref, down_ref)
    near = [2 * (i ^ (i >> 1)) + c for i in range(groups // 2) for c in range(2)]
    last = near[::-1]
    order = [(w, k) for w in range(2) for k in near] + [(2, k) for k in last]

    def peer(k):
        return jnp.bitwise_xor(f, k)

    def remote(source, target, send, recv, device):
        return pltpu.make_async_remote_copy(
            src_ref=source,
            dst_ref=target,
            send_sem=send,
            recv_sem=recv,
            device_id=device,
            device_id_type=MESH,
        )

    def load(k):
        return pltpu.make_async_copy(gate_ref.at[peer(k)], raw.at[0, peer(k)], load_sem.at[k])

    def bulk(w):
        return pltpu.make_async_copy(masters[w], raw.at[w], bulk_sem.at[w - 1])

    small = [
        pltpu.make_async_copy(source, target, small_sem.at[i])
        for i, (source, target) in enumerate(
            (
                (gain_ref, gain),
                (prompt_ref, prompt),
                (group_ref, group),
                (inner_ref, inner),
                (route_ref, route),
            )
        )
    ]

    def block(w, origin, k, begin=0, count=rows):
        first = pl.multiple_of(peer(k) * rows + begin, count)
        return served.at[w, origin, pl.ds(first, count)]

    def z_copy(w, k):
        device = {"fs": peer(k), "tp": t}
        return remote(cast.at[w, k - 1], block(w, t, 0), send_sem.at[2], zr.at[w, k - 1], device)

    def z_arrival(w, k):
        device = {"fs": peer(k), "tp": t}
        return remote(cast.at[w, k - 1], block(w, t, k), send_sem.at[2], zr.at[w, k - 1], device)

    def x_copy(s, origin):
        one = block(order[s][0], origin, order[s][1])
        return remote(one, one, send_sem.at[0], xr.at[s % groups], {"fs": f, "tp": tx})

    def y_copy(s, origin):
        one = block(order[s][0], origin, order[s][1])
        return remote(one, one, send_sem.at[1], yr.at[s % groups], {"fs": f, "tp": ty})

    def to_x(s):
        one = block(order[s][0], ty, order[s][1], half, half)
        return remote(one, one, send_sem.at[0], dr.at[s % groups], {"fs": f, "tp": tx})

    def to_y(s):
        one = block(order[s][0], tx, order[s][1], 0, half)
        return remote(one, one, send_sem.at[1], dr.at[s % groups], {"fs": f, "tp": ty})

    def diagonal_wait(s):
        one = block(order[s][0], td, order[s][1])
        remote(one, one, send_sem.at[0], dr.at[s % groups], {"fs": f, "tp": tx}).wait_recv()

    def part_copy(k):
        device = {"fs": peer(k), "tp": t}
        return remote(part.at[k - 1], got.at[k - 1], send_sem.at[3], pr, device)

    def side_start(s):
        x_copy(s, t).start()
        y_copy(s, t).start()

    def forward(s):
        x_copy(s, tx).wait_recv()
        to_y(s).start()
        y_copy(s, ty).wait_recv()
        to_x(s).start()

    def put(w, k, target):
        for e in range(per):
            value = raw[w, peer(k), e]
            if w < 2:
                value = value * scale[...]
            target[:, e * hidden : (e + 1) * hidden] = value.astype(jnp.bfloat16)

    def put_all(w):
        bulk(w).wait()
        put(w, 0, block(w, t, 0))

        def one(k, carry):
            put(w, k, cast.at[w, k - 1])
            return carry

        lax.fori_loop(1, groups, one, 0)

    def normalise():
        small[1].wait()
        values = prompt[...].astype(jnp.float32)
        mean = jnp.mean(values * values, axis=1, keepdims=True)
        normed[...] = (values * lax.rsqrt(mean + 1e-06)).astype(jnp.bfloat16)

    def columns():
        for i in range(2, 5):
            small[i].wait()
        chosen = group[...] * EPG + inner[...]
        for e in range(per):
            weight = jnp.sum(jnp.where(chosen == f * per + e, route[...], 0.0), axis=0, keepdims=True)
            column[:, e * hidden : (e + 1) * hidden] = jnp.broadcast_to(weight, (hidden, tokens)).T

    def hidden_units(origin):
        step = 2 * hidden
        for n in range(per // 2):
            at = pl.ds(n * step, step)
            scaled[origin, :, at] = activations(
                normed[...], served[0, origin, :, at], served[1, origin, :, at], column[:, at]
            )

    def features(k):
        total = None
        for i in range(parts):
            term = lax.dot_general(
                scaled[i],
                block(2, i, k)[...],
                (((1,), (1,)), ((), ())),
                preferred_element_type=jnp.float32,
            )
            total = term if total is None else total + term
        part[k - 1] = total.astype(jnp.bfloat16)

    small[0].start()
    load(0).start()
    barrier = pltpu.get_barrier_semaphore()
    for k in range(1, groups):
        pl.semaphore_signal(barrier, inc=1, device_id={"fs": peer(k), "tp": t}, device_id_type=MESH)
    for other in (tx, ty):
        pl.semaphore_signal(barrier, inc=1, device_id={"fs": f, "tp": other}, device_id_type=MESH)
    for k in near[1:]:
        load(k).start()
    for w in (1, 2):
        bulk(w).start()
    for copy in small[1:]:
        copy.start()
    small[0].wait()
    scale[...] = jnp.broadcast_to(gain[...], (hidden, rows)).T
    load(0).wait()
    put(0, 0, block(0, t, 0))
    load(near[1]).wait()
    put(0, near[1], cast.at[0, near[1] - 1])
    pl.semaphore_wait(barrier, groups + 1)
    side_start(0)
    for before, k in zip(near[1:], near[2:]):
        load(k).wait()
        put(0, k, cast.at[0, k - 1])
        z_copy(0, before).start()
    z_copy(0, last[0]).start()

    base, lag = 2 * groups, groups // 2
    sends = [(lag if i < 3 else lag + (i + 1) // 2, 1, k) for i, k in enumerate(near[1:])]
    sends += [(groups + 3 + i // 2, 2, k) for i, k in enumerate(last[:-1])]
    for s, (w, k) in enumerate(order):
        if s > 0:
            if k > 0:
                z_arrival(w, k).wait_recv()
            side_start(s)
            forward(s - 1)
        for at, array, one in sends:
            if at == s:
                z_copy(array, one).start()
        if s < 2:
            put_all(s + 1)
        if s == groups:
            normalise()
            columns()
        if 3 <= s < base + 2:
            diagonal_wait(s - 3)
        if s == base:
            hidden_units(t)
        if s == base + 1:
            hidden_units(tx)
            hidden_units(ty)
        if s == base + 2:
            diagonal_wait(base - 1)
            hidden_units(td)
        if s >= base + 2:
            diagonal_wait(s - 2)
            features(order[s - 2][1])
            part_copy(order[s - 2][1]).start()
    count = len(order)
    forward(count - 1)
    diagonal_wait(count - 2)
    features(1)
    part_copy(1).start()
    diagonal_wait(count - 1)
    sent = served.at[:, pl.ds(0, parts - 1), pl.ds(0, width // 2)]
    for i, whole in enumerate((sent, sent, cast, part)):
        remote(whole, whole, send_sem.at[i], pr, {"fs": f, "tp": tx}).wait_send()
    remote(got, got, send_sem.at[3], pr, {"fs": f, "tp": tx}).wait_recv()


def spread(prompt, norm_gain, gate_master, up_master, down_master, group_choice, inner_choice, route_weight):
    groups, parts = lax.axis_size("fs"), lax.axis_size("tp")
    experts, rows, hidden = gate_master.shape
    per = experts // groups
    tokens, width = prompt.shape
    arrays = 3
    views = [one.reshape(groups, per, rows, hidden) for one in (gate_master, up_master, down_master)]
    dma = pltpu.SemaphoreType.DMA
    return pl.pallas_call(
        spread_body,
        in_specs=[pl.BlockSpec(memory_space=pltpu.HBM)] * 8,
        out_specs=[pl.BlockSpec(memory_space=pltpu.VMEM)] * 3,
        out_shape=[
            pltpu.VMEM((arrays, parts, width, per * hidden), jnp.bfloat16),
            pltpu.VMEM((parts, tokens, per * hidden), jnp.bfloat16),
            pltpu.VMEM((groups - 1, tokens, rows), jnp.bfloat16),
        ],
        scratch_shapes=[
            pltpu.VMEM((arrays, groups, per, rows, hidden), jnp.float32),
            pltpu.VMEM((arrays, groups - 1, rows, per * hidden), jnp.bfloat16),
            pltpu.VMEM((1, rows), jnp.float32),
            pltpu.VMEM((rows, hidden), jnp.float32),
            pltpu.VMEM((tokens, width), jnp.bfloat16),
            pltpu.VMEM((tokens, width), jnp.bfloat16),
            pltpu.VMEM((1, tokens), jnp.int32),
            pltpu.VMEM((2, tokens), jnp.int32),
            pltpu.VMEM((2, tokens), jnp.float32),
            pltpu.VMEM((tokens, per * hidden), jnp.float32),
            pltpu.VMEM((groups - 1, tokens, rows), jnp.bfloat16),
            dma((groups,)),
            dma((2,)),
            dma((5,)),
            dma((4,)),
            dma((arrays, groups - 1)),
            dma((groups,)),
            dma((groups,)),
            dma((groups,)),
            dma,
        ],
        compiler_params=pltpu.CompilerParams(
            collective_id=0, has_side_effects=True, vmem_limit_bytes=32 * 1024 * 1024
        ),
        name="spread",
    )(
        norm_gain.reshape(1, rows),
        *views,
        prompt,
        group_choice.reshape(1, tokens),
        inner_choice.T,
        route_weight.T,
    )


def serve_body(served, scaled, got, gate_ref, up_ref, down_ref, mixed_ref, mixed, sem):
    arrays, parts, _, wide = served.shape
    rows = got.shape[2]
    hidden = FF // parts
    f = lax.axis_index("fs")
    outs = (gate_ref, up_ref, down_ref)
    for w, out in enumerate(outs):
        for i in range(parts):
            for e in range(wide // hidden):
                pltpu.make_async_copy(
                    served.at[w, i, :, pl.ds(e * hidden, hidden)],
                    out.at[:, pl.ds(e * FF + i * hidden, hidden)],
                    sem.at[w],
                ).start()
    total = None
    for i in range(parts):
        term = lax.dot_general(
            scaled[i],
            served[2, i, pl.ds(pl.multiple_of(f * rows, rows), rows), :],
            (((1,), (1,)), ((), ())),
            preferred_element_type=jnp.float32,
        )
        total = term if total is None else total + term
    for k in range(got.shape[0]):
        total = total + got[k].astype(jnp.float32)
    mixed[...] = (total * FF ** (-0.5)).astype(jnp.bfloat16)
    final = pltpu.make_async_copy(mixed, mixed_ref, sem.at[arrays])
    final.start()
    for w, out in enumerate(outs):
        pltpu.make_async_copy(out, out, sem.at[w]).wait()
    final.wait()


def serve(served, scaled, got):
    arrays, parts, width, wide = served.shape
    _, tokens, rows = got.shape
    out = jax.ShapeDtypeStruct((width, parts * wide), served.dtype)
    vmem, hbm = pl.BlockSpec(memory_space=pltpu.VMEM), pl.BlockSpec(memory_space=pltpu.HBM)
    return pl.pallas_call(
        serve_body,
        in_specs=[vmem, vmem, vmem],
        out_specs=[hbm, hbm, hbm, hbm],
        out_shape=[out, out, out, jax.ShapeDtypeStruct((tokens, rows), jnp.bfloat16)],
        scratch_shapes=[pltpu.VMEM((tokens, rows), jnp.bfloat16), pltpu.SemaphoreType.DMA((arrays + 1,))],
        compiler_params=pltpu.CompilerParams(vmem_limit_bytes=4 * 1024 * 1024),
        name="serve",
    )(*[pltpu.with_memory_space_constraint(one, pltpu.VMEM) for one in (served, scaled, got)])


def direct_shards(
    prompt, norm_gain, gate_master, up_master, down_master, group_choice, inner_choice, route_weight
):
    served, scaled, got = spread(
        prompt, norm_gain, gate_master, up_master, down_master, group_choice, inner_choice, route_weight
    )
    return tuple(serve(served, scaled, got))


def fits_direct(mesh):
    groups, parts = mesh.shape["fs"], mesh.shape["tp"]
    whole_experts = (GROUPS * EPG) % groups == 0 and (GROUPS * EPG // groups) % 2 == 0
    return parts == 4 and groups >= 4 and groups & (groups - 1) == 0 and whole_experts and FF // parts % 128 == 0


def solution(mesh):
    in_specs = (
        P("tp", None),
        P("fs"),
        P(None, "fs", "tp"),
        P(None, "fs", "tp"),
        P(None, "fs", "tp"),
        P("tp"),
        P("tp", None),
        P("tp", None),
    )
    out_specs = (P(None, "fs"), P(None, "fs"), P(None, "fs"), P("tp", "fs"))
    body = direct_shards if fits_direct(mesh) else shards
    return jax.shard_map(body, mesh=mesh, in_specs=in_specs, out_specs=out_specs, check_vma=False)
```

```python
import jax
import jax.numpy as jnp
from jax import lax
from jax.experimental import pallas as pl
from jax.experimental.pallas import tpu as pltpu
from jax.sharding import PartitionSpec as P

MESH = pl.DeviceIdType.MESH
FF = 512
GROUPS = 4
EPG = 8


def flatten_rows(piece):
    count, experts, rows, hidden = piece.shape
    return piece.transpose(0, 2, 1, 3).reshape(count, rows, experts * hidden)


def restore_rows(gathered, rows):
    parts = lax.axis_size("tp")
    count, total, width = gathered.shape
    blocks = total // (parts * rows)
    ordered = gathered.reshape(count, parts, blocks, rows, width).transpose(0, 2, 1, 3, 4)
    return ordered.reshape(count, total, width)


def activations(normed, gate_local, up_local, column_weight):
    width = normed.shape[1]
    gate_act = jnp.dot(normed, gate_local, preferred_element_type=jnp.float32) * width ** (-0.5)
    up_act = jnp.dot(normed, up_local, preferred_element_type=jnp.float32) * width ** (-0.5)
    return (column_weight * jax.nn.silu(gate_act) * up_act).astype(jnp.bfloat16)


def route_columns(weight, columns, experts):
    first = lax.axis_index("fs") * columns
    owner = (first + jnp.arange(columns, dtype=jnp.int32)) // FF
    onehot = (owner[None, :] == jnp.arange(experts, dtype=jnp.int32)[:, None]).astype(jnp.float32)
    return jnp.dot(weight, onehot, precision=lax.Precision.HIGHEST)


def shards(
    prompt, norm_gain, gate_master, up_master, down_master, group_choice, inner_choice, route_weight
):
    experts = GROUPS * EPG
    scale = norm_gain[None, :, None]
    gate_cast = (gate_master * scale).astype(jnp.bfloat16)
    up_cast = (up_master * scale).astype(jnp.bfloat16)
    down_cast = down_master.astype(jnp.bfloat16)
    rows = gate_master.shape[1] // lax.axis_size("tp")
    values = prompt.astype(jnp.float32)
    normed = (values * lax.rsqrt(jnp.mean(values * values, axis=1, keepdims=True) + 1e-06)).astype(
        jnp.bfloat16
    )
    chosen = group_choice[:, None] * EPG + inner_choice
    member = (chosen[:, :, None] == jnp.arange(experts, dtype=jnp.int32)[None, None, :]).astype(
        jnp.float32
    )
    weight = jnp.sum(member * route_weight[:, :, None], axis=1)
    stacked = jnp.stack([gate_cast, up_cast, down_cast])
    widened = lax.all_to_all(stacked, "tp", split_axis=2, concat_axis=3, tiled=True)
    moved = lax.all_to_all(flatten_rows(widened), "fs", split_axis=2, concat_axis=1, tiled=True)
    served = restore_rows(lax.all_gather(moved, "tp", axis=1, tiled=True), rows)
    gate_local, up_local, down_local = (served[0], served[1], served[2])
    column_weight = route_columns(weight, gate_local.shape[1], experts)
    scaled = activations(normed, gate_local, up_local, column_weight)
    summed = lax.psum_scatter(
        lax.dot_general(
            down_local, scaled, (((1,), (1,)), ((), ())), preferred_element_type=jnp.float32
        ),
        "fs",
        scatter_dimension=0,
        tiled=True,
    )
    mixed = (summed * FF ** (-0.5)).T.astype(jnp.bfloat16)
    return (gate_local, up_local, down_local, mixed)


def remote(source, target, send, recv, device):
    return pltpu.make_async_remote_copy(
        src_ref=source,
        dst_ref=target,
        send_sem=send,
        recv_sem=recv,
        device_id=device,
        device_id_type=MESH,
    )


def block_order(groups):
    near = [2 * (i ^ (i >> 1)) + c for i in range(groups // 2) for c in range(2)]
    last = near[::-1]
    return near, [k for k in last if k % 2 == 1], [k for k in last if k % 2 == 0]


def matmul_nt(left, right):
    return lax.dot_general(left, right, (((1,), (1,)), ((), ())), preferred_element_type=jnp.float32)


def spread_body(
    gain_ref,
    gate_ref,
    up_ref,
    down_ref,
    prompt_ref,
    group_ref,
    inner_ref,
    route_ref,
    wide,
    down,
    scaled,
    got,
    raw,
    cast,
    gain,
    scale,
    prompt,
    normed,
    group,
    inner,
    route,
    column,
    part,
    load_sem,
    bulk_sem,
    small_sem,
    send_sem,
    zr,
    xr,
    yr,
    dr,
    pr,
):
    f, t = lax.axis_index("fs"), lax.axis_index("tp")
    tx, ty, td = jnp.bitwise_xor(t, 1), jnp.bitwise_xor(t, 2), jnp.bitwise_xor(t, 3)
    arrays, groups, per, rows, hidden = raw.shape
    parts, width = down.shape[:2]
    tokens = prompt.shape[0]
    half = rows // 2
    masters = (gate_ref, up_ref, down_ref)
    near, odds, evens = block_order(groups)
    order = [(w, k) for w in range(2) for k in near] + [(2, k) for k in odds + evens]
    base, split, lag = 2 * groups, 2 * groups + len(odds), groups // 2

    def peer(k):
        return jnp.bitwise_xor(f, k)

    def load(k):
        return pltpu.make_async_copy(gate_ref.at[peer(k)], raw.at[0, peer(k)], load_sem.at[k])

    def bulk(w):
        return pltpu.make_async_copy(masters[w], raw.at[w], bulk_sem.at[w - 1])

    small = [
        pltpu.make_async_copy(source, target, small_sem.at[i])
        for i, (source, target) in enumerate(
            (
                (gain_ref, gain),
                (prompt_ref, prompt),
                (group_ref, group),
                (inner_ref, inner),
                (route_ref, route),
            )
        )
    ]

    def block(w, origin, k, begin=0, count=rows):
        at = pl.ds(pl.multiple_of(peer(k) * rows + begin, count), count)
        return wide.at[w, origin, at] if w < 2 else down.at[origin, at]

    def z_copy(w, k):
        device = {"fs": peer(k), "tp": t}
        return remote(cast.at[w, k - 1], block(w, t, 0), send_sem.at[4], zr.at[w, k - 1], device)

    def z_arrival(w, k):
        device = {"fs": peer(k), "tp": t}
        return remote(cast.at[w, k - 1], block(w, t, k), send_sem.at[4], zr.at[w, k - 1], device)

    def x_copy(s, origin):
        one = block(order[s][0], origin, order[s][1])
        return remote(one, one, send_sem.at[s // base], xr.at[s % groups], {"fs": f, "tp": tx})

    def y_copy(s, origin):
        one = block(order[s][0], origin, order[s][1])
        return remote(one, one, send_sem.at[2 + s // base], yr.at[s % groups], {"fs": f, "tp": ty})

    def to_x(s):
        one = block(order[s][0], ty, order[s][1], half, half)
        return remote(one, one, send_sem.at[s // base], dr.at[s % groups], {"fs": f, "tp": tx})

    def to_y(s):
        one = block(order[s][0], tx, order[s][1], 0, half)
        return remote(one, one, send_sem.at[2 + s // base], dr.at[s % groups], {"fs": f, "tp": ty})

    def diagonal_wait(s):
        one = block(order[s][0], td, order[s][1])
        remote(one, one, send_sem.at[0], dr.at[s % groups], {"fs": f, "tp": tx}).wait_recv()

    def side_start(s):
        x_copy(s, t).start()
        y_copy(s, t).start()

    def forward(s):
        x_copy(s, tx).wait_recv()
        to_y(s).start()
        y_copy(s, ty).wait_recv()
        to_x(s).start()

    def put(w, k, target):
        for e in range(per):
            value = raw[w, peer(k), e]
            if w < 2:
                value = value * scale[...]
            target[:, e * hidden : (e + 1) * hidden] = value.astype(jnp.bfloat16)

    def put_all(w):
        bulk(w).wait()
        put(w, 0, block(w, t, 0))

        def one(k, carry):
            put(w, k, cast.at[w, k - 1])
            return carry

        lax.fori_loop(1, groups, one, 0)

    def normalise():
        small[1].wait()
        values = prompt[...].astype(jnp.float32)
        mean = jnp.mean(values * values, axis=1, keepdims=True)
        normed[...] = (values * lax.rsqrt(mean + 1e-06)).astype(jnp.bfloat16)

    def columns():
        for i in range(2, 5):
            small[i].wait()
        chosen = group[...] * EPG + inner[...]
        for e in range(per):
            weight = jnp.sum(jnp.where(chosen == f * per + e, route[...], 0.0), axis=0, keepdims=True)
            column[:, e * hidden : (e + 1) * hidden] = jnp.broadcast_to(weight, (hidden, tokens)).T

    def hidden_units(origin):
        step = 2 * hidden
        for n in range(per // 2):
            at = pl.ds(n * step, step)
            scaled[origin, :, at] = activations(
                normed[...], wide[0, origin, :, at], wide[1, origin, :, at], column[:, at]
            )

    def features(s):
        k = order[s][1]
        diagonal_wait(s)
        total = matmul_nt(scaled[0], block(2, 0, k)[...])
        for i in range(1, parts):
            total = total + matmul_nt(scaled[i], block(2, i, k)[...])
        part[s - base] = total.astype(jnp.bfloat16)
        device = {"fs": peer(k), "tp": t}
        remote(part.at[s - base], got.at[k - 1], send_sem.at[5], pr, device).start()

    small[0].start()
    load(0).start()
    barrier = pltpu.get_barrier_semaphore()
    for k in range(1, groups):
        pl.semaphore_signal(barrier, inc=1, device_id={"fs": peer(k), "tp": t}, device_id_type=MESH)
    for other in (tx, ty):
        pl.semaphore_signal(barrier, inc=1, device_id={"fs": f, "tp": other}, device_id_type=MESH)
    for k in near[1:]:
        load(k).start()
    for w in (1, 2):
        bulk(w).start()
    for copy in small[1:]:
        copy.start()
    small[0].wait()
    scale[...] = jnp.broadcast_to(gain[...], (hidden, rows)).T
    load(0).wait()
    put(0, 0, block(0, t, 0))
    load(near[1]).wait()
    put(0, near[1], cast.at[0, near[1] - 1])
    pl.semaphore_wait(barrier, groups + 1)
    side_start(0)
    for before, k in zip(near[1:], near[2:]):
        load(k).wait()
        put(0, k, cast.at[0, k - 1])
        z_copy(0, before).start()
    z_copy(0, near[-1]).start()

    sends = [(lag if i < 3 else lag + (i + 1) // 2, 1, k) for i, k in enumerate(near[1:])]
    sends += [(groups + 3 + i // 2, 2, k) for i, k in enumerate(near[:0:-1])]

    def step(s):
        w, k = order[s]
        if s > 0:
            if k > 0:
                z_arrival(w, k).wait_recv()
            side_start(s)
            forward(s - 1)
        for at, array, one in sends:
            if at == s:
                z_copy(array, one).start()
        if s < 2:
            put_all(s + 1)
        if s == groups:
            normalise()
            columns()
        if 3 <= s < base + 2:
            diagonal_wait(s - 3)
        if s == base:
            hidden_units(t)
        if s == base + 1:
            hidden_units(tx)
            hidden_units(ty)
        if s == base + 2:
            diagonal_wait(base - 1)
            hidden_units(td)
        if s >= base + 2:
            features(s - 2)

    def drain(end):
        forward(end - 1)
        features(end - 2)
        if order[end - 1][1] > 0:
            features(end - 1)
        else:
            diagonal_wait(end - 1)
        count = end - base
        sums = min(count, groups - 1)
        first = wide.at[:, pl.ds(0, parts - 1), pl.ds(0, width // 2)]
        second = down.at[pl.ds(0, parts - 1), pl.ds(0, count * half)]
        for i, whole in enumerate((first, second, first, second, cast, part.at[pl.ds(0, sums)])):
            remote(whole, whole, send_sem.at[i], pr, {"fs": f, "tp": tx}).wait_send()
        whole = got.at[pl.ds(0, sums)]
        remote(whole, whole, send_sem.at[5], pr, {"fs": f, "tp": tx}).wait_recv()

    for s in range(split):
        step(s)

    @pl.when(f % 2 == 0)
    def _():
        for k in evens[:-1]:
            z_arrival(2, k).wait_recv()
        drain(split)

    @pl.when(f % 2 == 1)
    def _():
        for s in range(split, len(order)):
            step(s)
        drain(len(order))


def spread(prompt, norm_gain, gate_master, up_master, down_master, group_choice, inner_choice, route_weight):
    groups, parts = lax.axis_size("fs"), lax.axis_size("tp")
    experts, rows, hidden = gate_master.shape
    per = experts // groups
    tokens, width = prompt.shape
    arrays = 3
    views = [one.reshape(groups, per, rows, hidden) for one in (gate_master, up_master, down_master)]
    dma = pltpu.SemaphoreType.DMA
    return pl.pallas_call(
        spread_body,
        in_specs=[pl.BlockSpec(memory_space=pltpu.HBM)] * 8,
        out_specs=[pl.BlockSpec(memory_space=pltpu.VMEM)] * 4,
        out_shape=[
            pltpu.VMEM((2, parts, width, per * hidden), jnp.bfloat16),
            pltpu.VMEM((parts, width, per * hidden), jnp.bfloat16),
            pltpu.VMEM((parts, tokens, per * hidden), jnp.bfloat16),
            pltpu.VMEM((groups - 1, tokens, rows), jnp.bfloat16),
        ],
        scratch_shapes=[
            pltpu.VMEM((arrays, groups, per, rows, hidden), jnp.float32),
            pltpu.VMEM((arrays, groups - 1, rows, per * hidden), jnp.bfloat16),
            pltpu.VMEM((1, rows), jnp.float32),
            pltpu.VMEM((rows, hidden), jnp.float32),
            pltpu.VMEM((tokens, width), jnp.bfloat16),
            pltpu.VMEM((tokens, width), jnp.bfloat16),
            pltpu.VMEM((1, tokens), jnp.int32),
            pltpu.VMEM((2, tokens), jnp.int32),
            pltpu.VMEM((2, tokens), jnp.float32),
            pltpu.VMEM((tokens, per * hidden), jnp.float32),
            pltpu.VMEM((groups - 1, tokens, rows), jnp.bfloat16),
            dma((groups,)),
            dma((2,)),
            dma((5,)),
            dma((6,)),
            dma((arrays, groups - 1)),
            dma((groups,)),
            dma((groups,)),
            dma((groups,)),
            dma,
        ],
        compiler_params=pltpu.CompilerParams(
            collective_id=0, has_side_effects=True, vmem_limit_bytes=32 * 1024 * 1024
        ),
        name="spread",
    )(
        norm_gain.reshape(1, rows),
        *views,
        prompt,
        group_choice.reshape(1, tokens),
        inner_choice.T,
        route_weight.T,
    )


def store_body(wide, down, gate_ref, up_ref, down_ref, token_ref, sem):
    parts, width, hold = down.shape
    hidden = FF // parts
    groups, per = lax.axis_size("fs"), hold // hidden
    rows = width // groups
    f = lax.axis_index("fs")
    _, odds, evens = block_order(groups)

    def put(k):
        at = pl.ds(pl.multiple_of(jnp.bitwise_xor(f, k) * rows, rows), rows)
        for i in range(parts):
            for e in range(per):
                pltpu.make_async_copy(
                    down.at[i, at, pl.ds(e * hidden, hidden)],
                    down_ref.at[at, pl.ds(e * FF + i * hidden, hidden)],
                    sem.at[2],
                ).start()

    def wait(count):
        done = down_ref.at[pl.ds(0, count * rows)]
        pltpu.make_async_copy(done, done, sem.at[2]).wait()

    outs = (gate_ref, up_ref)
    for w, out in enumerate(outs):
        for i in range(parts):
            for e in range(per):
                pltpu.make_async_copy(
                    wide.at[w, i, :, pl.ds(e * hidden, hidden)],
                    out.at[:, pl.ds(e * FF + i * hidden, hidden)],
                    sem.at[w],
                ).start()
    for k in odds:
        put(k)

    @pl.when(f % 2 == 1)
    def _():
        for k in evens:
            put(k)
        wait(groups)

    @pl.when(f % 2 == 0)
    def _():
        wait(len(odds))

    for w, out in enumerate(outs):
        pltpu.make_async_copy(out, out, sem.at[w]).wait()


def hold_in_vmem(*arrays):
    return [pltpu.with_memory_space_constraint(one, pltpu.VMEM) for one in arrays]


def store(wide, down):
    parts, width, hold = down.shape
    out = pltpu.HBM((width, parts * hold), down.dtype)
    vmem, hbm = pl.BlockSpec(memory_space=pltpu.VMEM), pl.BlockSpec(memory_space=pltpu.HBM)
    return pl.pallas_call(
        store_body,
        in_specs=[vmem, vmem],
        out_specs=[hbm, hbm, hbm, hbm],
        out_shape=[out, out, out, pltpu.HBM((8, 128), jnp.float32)],
        scratch_shapes=[pltpu.SemaphoreType.DMA((3,))],
        compiler_params=pltpu.CompilerParams(vmem_limit_bytes=4 * 1024 * 1024),
        name="store",
    )(*hold_in_vmem(wide, down))


def finish_body(down, scaled, got, token_ref, late, got_late, mine, part, send_sem, xr, yr, dr, pr):
    f, t = lax.axis_index("fs"), lax.axis_index("tp")
    tx, ty = jnp.bitwise_xor(t, 1), jnp.bitwise_xor(t, 2)
    parts = down.shape[0]
    rows = late.shape[2]
    half, quarter = rows // 2, rows // 4
    _, odds, evens = block_order(lax.axis_size("fs"))
    count = len(evens)

    def own(i, begin=0, size=rows):
        first = jnp.bitwise_xor(f, evens[i]) * rows + begin
        return down.at[t, pl.ds(pl.multiple_of(first, size), size)]

    def landed(j, q, begin=0, size=half):
        return late.at[j, q // 2, pl.ds(q % 2 * half + begin, size)]

    def x_copy(q):
        source = own(q // 2, q % 2 * half, half)
        return remote(source, landed(0, q), send_sem.at[0], xr.at[q], {"fs": f, "tp": tx})

    def y_copy(q):
        source = own(q // 2, q % 2 * half, half)
        return remote(source, landed(1, q), send_sem.at[1], yr.at[q], {"fs": f, "tp": ty})

    def to_y(q):
        source, target = landed(0, q, 0, quarter), landed(2, q, 0, quarter)
        return remote(source, target, send_sem.at[1], dr.at[q], {"fs": f, "tp": ty})

    def to_x(q):
        source, target = landed(1, q, quarter, quarter), landed(2, q, quarter, quarter)
        return remote(source, target, send_sem.at[0], dr.at[q], {"fs": f, "tp": tx})

    def side_start(q):
        x_copy(q).start()
        y_copy(q).start()

    def forward(q):
        x_copy(q).wait_recv()
        to_y(q).start()
        y_copy(q).wait_recv()
        to_x(q).start()

    def straight(i):
        total = matmul_nt(scaled[t], own(i)[...])
        for j in (1, 2):
            total = total + matmul_nt(scaled[jnp.bitwise_xor(t, j)], late[j - 1, i])
        return total

    def diagonal(i):
        for q in (2 * i, 2 * i + 1):
            one = landed(2, q)
            remote(one, one, send_sem.at[0], dr.at[q], {"fs": f, "tp": tx}).wait_recv()
        return matmul_nt(scaled[jnp.bitwise_xor(t, 3)], late[2, i])

    def features(i):
        mine[...] = straight(i)
        part[i] = (mine[...] + diagonal(i)).astype(jnp.bfloat16)
        device = {"fs": jnp.bitwise_xor(f, evens[i]), "tp": t}
        remote(part.at[i], got_late.at[i], send_sem.at[2], pr, device).start()

    def collected(total, chosen):
        for k in chosen:
            total = total + got[k - 1].astype(jnp.float32)
        return total

    def run():
        ahead, chunks = 4, 2 * count
        for q in range(ahead):
            side_start(q)
        sent = ahead
        for q in range(chunks):
            forward(q)
            if sent < chunks - 2 or (q % 2 == 1 and sent < chunks):
                side_start(sent)
                sent += 1
            if q % 2 == 1 and 3 <= q < chunks - 1:
                features((q - 3) // 2)
            if q == chunks - 2:
                features(count - 2)
        mine[...] = collected(straight(count - 1), odds)
        mine[...] += diagonal(count - 1)
        sides = late.at[:, :, pl.ds(0, half)]
        for i, whole in enumerate((sides, sides, part)):
            remote(whole, whole, send_sem.at[i], pr, {"fs": f, "tp": tx}).wait_send()
        remote(got_late, got_late, send_sem.at[2], pr, {"fs": f, "tp": tx}).wait_recv()

    @pl.when(f % 2 == 0)
    def _():
        barrier = pltpu.get_barrier_semaphore()
        others = [{"fs": jnp.bitwise_xor(f, k), "tp": t} for k in evens[:-1]]
        others += [{"fs": f, "tp": tx}, {"fs": f, "tp": ty}]
        for other in others:
            pl.semaphore_signal(barrier, inc=1, device_id=other, device_id_type=MESH)
        pl.semaphore_wait(barrier, len(others))
        run()

    @pl.when(f % 2 == 1)
    def _():
        at = pl.ds(pl.multiple_of(f * rows, rows), rows)
        total = matmul_nt(scaled[0], down[0, at, :])
        for i in range(1, parts):
            total = total + matmul_nt(scaled[i], down[i, at, :])
        mine[...] = collected(total, odds + evens[:-1])


def finish(down, scaled, got, token, groups):
    parts, width, hold = down.shape
    tokens, rows, count = scaled.shape[1], width // groups, groups // 2
    vmem, hbm = pl.BlockSpec(memory_space=pltpu.VMEM), pl.BlockSpec(memory_space=pltpu.HBM)
    dma = pltpu.SemaphoreType.DMA
    return pl.pallas_call(
        finish_body,
        in_specs=[vmem, vmem, vmem, hbm],
        out_specs=[vmem, vmem, vmem],
        out_shape=[
            pltpu.VMEM((parts - 1, count, rows, hold), down.dtype),
            pltpu.VMEM((count - 1, tokens, rows), jnp.bfloat16),
            pltpu.VMEM((tokens, rows), jnp.float32),
        ],
        scratch_shapes=[
            pltpu.VMEM((count - 1, tokens, rows), jnp.bfloat16),
            dma((3,)),
            dma((2 * count,)),
            dma((2 * count,)),
            dma((2 * count,)),
            dma,
        ],
        compiler_params=pltpu.CompilerParams(
            collective_id=1, has_side_effects=True, vmem_limit_bytes=4 * 1024 * 1024
        ),
        name="finish",
    )(*hold_in_vmem(down, scaled, got), pltpu.with_memory_space_constraint(token, pltpu.HBM))


def serve_body(down, late, got_late, mine, down_in, down_ref, mixed_ref, mixed, sem):
    parts, width, hold = down.shape
    hidden, rows = FF // parts, late.shape[2]
    f, t = lax.axis_index("fs"), lax.axis_index("tp")
    _, _, evens = block_order(width // rows)
    count = len(evens)

    def put(i):
        at = pl.ds(pl.multiple_of(jnp.bitwise_xor(f, evens[i]) * rows, rows), rows)
        for j in range(parts):
            origin = jnp.bitwise_xor(t, j)
            source = late.at[j - 1, i] if j > 0 else down.at[t, at]
            for e in range(hold // hidden):
                begin = pl.multiple_of(e * FF + origin * hidden, hidden)
                pltpu.make_async_copy(
                    source.at[:, pl.ds(e * hidden, hidden)], down_ref.at[at, pl.ds(begin, hidden)], sem.at[0]
                ).start()

    def finish_mixed(total):
        mixed[...] = (total * FF ** (-0.5)).astype(jnp.bfloat16)
        final = pltpu.make_async_copy(mixed, mixed_ref, sem.at[1])
        final.start()
        return final

    @pl.when(f % 2 == 0)
    def _():
        for i in range(count):
            put(i)
        total = mine[...]
        for i in range(count - 1):
            total = total + got_late[i].astype(jnp.float32)
        final = finish_mixed(total)
        done = down_ref.at[pl.ds(0, count * rows)]
        pltpu.make_async_copy(done, done, sem.at[0]).wait()
        final.wait()

    @pl.when(f % 2 == 1)
    def _():
        finish_mixed(mine[...]).wait()


def serve(down, late, got_late, mine, down_out):
    tokens, rows = mine.shape
    vmem, hbm = pl.BlockSpec(memory_space=pltpu.VMEM), pl.BlockSpec(memory_space=pltpu.HBM)
    return pl.pallas_call(
        serve_body,
        in_specs=[vmem] * 4 + [hbm],
        out_specs=[hbm, hbm],
        out_shape=[pltpu.HBM(down_out.shape, down_out.dtype), pltpu.HBM((tokens, rows), jnp.bfloat16)],
        input_output_aliases={4: 0},
        scratch_shapes=[pltpu.VMEM((tokens, rows), jnp.bfloat16), pltpu.SemaphoreType.DMA((2,))],
        compiler_params=pltpu.CompilerParams(vmem_limit_bytes=4 * 1024 * 1024),
        name="serve",
    )(*hold_in_vmem(down, late, got_late, mine), pltpu.with_memory_space_constraint(down_out, pltpu.HBM))


def direct_shards(
    prompt, norm_gain, gate_master, up_master, down_master, group_choice, inner_choice, route_weight
):
    groups = lax.axis_size("fs")
    wide, down, scaled, got = spread(
        prompt, norm_gain, gate_master, up_master, down_master, group_choice, inner_choice, route_weight
    )
    gate_local, up_local, down_some, token = store(wide, down)
    late, got_late, mine = finish(down, scaled, got, token, groups)
    down_local, mixed = serve(down, late, got_late, mine, down_some)
    return (gate_local, up_local, down_local, mixed)


def fits_direct(mesh):
    groups, parts = mesh.shape["fs"], mesh.shape["tp"]
    whole_experts = (GROUPS * EPG) % groups == 0 and (GROUPS * EPG // groups) % 2 == 0
    return parts == 4 and groups >= 4 and groups & (groups - 1) == 0 and whole_experts and FF // parts % 128 == 0


def solution(mesh):
    in_specs = (
        P("tp", None),
        P("fs"),
        P(None, "fs", "tp"),
        P(None, "fs", "tp"),
        P(None, "fs", "tp"),
        P("tp"),
        P("tp", None),
        P("tp", None),
    )
    out_specs = (P(None, "fs"), P(None, "fs"), P(None, "fs"), P("tp", "fs"))
    body = direct_shards if fits_direct(mesh) else shards
    return jax.shard_map(body, mesh=mesh, in_specs=in_specs, out_specs=out_specs, check_vma=False)
```

```python
import jax
import jax.numpy as jnp
from jax import lax
from jax.experimental import pallas as pl
from jax.experimental.pallas import tpu as pltpu
from jax.sharding import PartitionSpec as P

MESH = pl.DeviceIdType.MESH
FF = 512
GROUPS = 4
EPG = 8


def flatten_rows(piece):
    count, experts, rows, hidden = piece.shape
    return piece.transpose(0, 2, 1, 3).reshape(count, rows, experts * hidden)


def restore_rows(gathered, rows):
    parts = lax.axis_size("tp")
    count, total, width = gathered.shape
    blocks = total // (parts * rows)
    ordered = gathered.reshape(count, parts, blocks, rows, width).transpose(0, 2, 1, 3, 4)
    return ordered.reshape(count, total, width)


def activations(normed, gate_local, up_local, column_weight):
    width = normed.shape[1]
    gate_act = jnp.dot(normed, gate_local, preferred_element_type=jnp.float32) * width ** (-0.5)
    up_act = jnp.dot(normed, up_local, preferred_element_type=jnp.float32) * width ** (-0.5)
    return (column_weight * jax.nn.silu(gate_act) * up_act).astype(jnp.bfloat16)


def route_columns(weight, columns, experts):
    first = lax.axis_index("fs") * columns
    owner = (first + jnp.arange(columns, dtype=jnp.int32)) // FF
    onehot = (owner[None, :] == jnp.arange(experts, dtype=jnp.int32)[:, None]).astype(jnp.float32)
    return jnp.dot(weight, onehot, precision=lax.Precision.HIGHEST)


def shards(
    prompt, norm_gain, gate_master, up_master, down_master, group_choice, inner_choice, route_weight
):
    experts = GROUPS * EPG
    scale = norm_gain[None, :, None]
    gate_cast = (gate_master * scale).astype(jnp.bfloat16)
    up_cast = (up_master * scale).astype(jnp.bfloat16)
    down_cast = down_master.astype(jnp.bfloat16)
    rows = gate_master.shape[1] // lax.axis_size("tp")
    values = prompt.astype(jnp.float32)
    normed = (values * lax.rsqrt(jnp.mean(values * values, axis=1, keepdims=True) + 1e-06)).astype(
        jnp.bfloat16
    )
    chosen = group_choice[:, None] * EPG + inner_choice
    member = (chosen[:, :, None] == jnp.arange(experts, dtype=jnp.int32)[None, None, :]).astype(
        jnp.float32
    )
    weight = jnp.sum(member * route_weight[:, :, None], axis=1)
    stacked = jnp.stack([gate_cast, up_cast, down_cast])
    widened = lax.all_to_all(stacked, "tp", split_axis=2, concat_axis=3, tiled=True)
    moved = lax.all_to_all(flatten_rows(widened), "fs", split_axis=2, concat_axis=1, tiled=True)
    served = restore_rows(lax.all_gather(moved, "tp", axis=1, tiled=True), rows)
    gate_local, up_local, down_local = (served[0], served[1], served[2])
    column_weight = route_columns(weight, gate_local.shape[1], experts)
    scaled = activations(normed, gate_local, up_local, column_weight)
    summed = lax.psum_scatter(
        lax.dot_general(
            down_local, scaled, (((1,), (1,)), ((), ())), preferred_element_type=jnp.float32
        ),
        "fs",
        scatter_dimension=0,
        tiled=True,
    )
    mixed = (summed * FF ** (-0.5)).T.astype(jnp.bfloat16)
    return (gate_local, up_local, down_local, mixed)


def remote(source, target, send, recv, device):
    return pltpu.make_async_remote_copy(
        src_ref=source,
        dst_ref=target,
        send_sem=send,
        recv_sem=recv,
        device_id=device,
        device_id_type=MESH,
    )


def block_order(groups):
    near = [2 * (i ^ (i >> 1)) + c for i in range(groups // 2) for c in range(2)]
    last = near[::-1]
    return near, [k for k in last if k % 2 == 1], [k for k in last if k % 2 == 0]


def matmul_nt(left, right):
    return lax.dot_general(left, right, (((1,), (1,)), ((), ())), preferred_element_type=jnp.float32)


def spread_body(
    gain_ref,
    gate_ref,
    up_ref,
    down_ref,
    prompt_ref,
    group_ref,
    inner_ref,
    route_ref,
    wide,
    down,
    scaled,
    got,
    raw,
    cast,
    gain,
    scale,
    prompt,
    normed,
    group,
    inner,
    route,
    column,
    part,
    load_sem,
    bulk_sem,
    small_sem,
    send_sem,
    zr,
    xr,
    yr,
    dr,
    pr,
):
    f, t = lax.axis_index("fs"), lax.axis_index("tp")
    tx, ty, td = jnp.bitwise_xor(t, 1), jnp.bitwise_xor(t, 2), jnp.bitwise_xor(t, 3)
    arrays, groups, per, rows, hidden = raw.shape
    parts, width = down.shape[:2]
    tokens = prompt.shape[0]
    half = rows // 2
    masters = (gate_ref, up_ref, down_ref)
    near, odds, evens = block_order(groups)
    order = [(w, k) for w in range(2) for k in near] + [(2, k) for k in odds + evens]
    base, split, lag = 2 * groups, 2 * groups + len(odds), groups // 2

    def peer(k):
        return jnp.bitwise_xor(f, k)

    def load(k):
        return pltpu.make_async_copy(gate_ref.at[peer(k)], raw.at[0, peer(k)], load_sem.at[k])

    def bulk(w):
        return pltpu.make_async_copy(masters[w], raw.at[w], bulk_sem.at[w - 1])

    small = [
        pltpu.make_async_copy(source, target, small_sem.at[i])
        for i, (source, target) in enumerate(
            (
                (gain_ref, gain),
                (prompt_ref, prompt),
                (group_ref, group),
                (inner_ref, inner),
                (route_ref, route),
            )
        )
    ]

    def block(w, origin, k, begin=0, count=rows):
        at = pl.ds(pl.multiple_of(peer(k) * rows + begin, count), count)
        return wide.at[w, origin, at] if w < 2 else down.at[origin, at]

    def z_copy(w, k):
        device = {"fs": peer(k), "tp": t}
        return remote(cast.at[w, k - 1], block(w, t, 0), send_sem.at[4], zr.at[w, k - 1], device)

    def z_arrival(w, k):
        device = {"fs": peer(k), "tp": t}
        return remote(cast.at[w, k - 1], block(w, t, k), send_sem.at[4], zr.at[w, k - 1], device)

    def x_copy(s, origin):
        one = block(order[s][0], origin, order[s][1])
        return remote(one, one, send_sem.at[s // base], xr.at[s % groups], {"fs": f, "tp": tx})

    def y_copy(s, origin):
        one = block(order[s][0], origin, order[s][1])
        return remote(one, one, send_sem.at[2 + s // base], yr.at[s % groups], {"fs": f, "tp": ty})

    def to_x(s):
        one = block(order[s][0], ty, order[s][1], half, half)
        return remote(one, one, send_sem.at[s // base], dr.at[s % groups], {"fs": f, "tp": tx})

    def to_y(s):
        one = block(order[s][0], tx, order[s][1], 0, half)
        return remote(one, one, send_sem.at[2 + s // base], dr.at[s % groups], {"fs": f, "tp": ty})

    def diagonal_wait(s):
        one = block(order[s][0], td, order[s][1])
        remote(one, one, send_sem.at[0], dr.at[s % groups], {"fs": f, "tp": tx}).wait_recv()

    def side_start(s):
        x_copy(s, t).start()
        y_copy(s, t).start()

    def side_half(s, begin):
        one = block(order[s][0], t, order[s][1], begin, half)
        remote(one, one, send_sem.at[s // base], xr.at[s % groups], {"fs": f, "tp": tx}).start()
        remote(one, one, send_sem.at[2 + s // base], yr.at[s % groups], {"fs": f, "tp": ty}).start()

    def forward(s):
        x_copy(s, tx).wait_recv()
        to_y(s).start()
        y_copy(s, ty).wait_recv()
        to_x(s).start()

    def put(w, k, target):
        for e in range(per):
            value = raw[w, peer(k), e]
            if w < 2:
                value = value * scale[...]
            target[:, e * hidden : (e + 1) * hidden] = value.astype(jnp.bfloat16)

    def put_all(w):
        bulk(w).wait()
        put(w, 0, block(w, t, 0))

        def one(k, carry):
            put(w, k, cast.at[w, k - 1])
            return carry

        lax.fori_loop(1, groups, one, 0)

    def normalise():
        small[1].wait()
        values = prompt[...].astype(jnp.float32)
        mean = jnp.mean(values * values, axis=1, keepdims=True)
        normed[...] = (values * lax.rsqrt(mean + 1e-06)).astype(jnp.bfloat16)

    def columns():
        for i in range(2, 5):
            small[i].wait()
        chosen = group[...] * EPG + inner[...]
        for e in range(per):
            weight = jnp.sum(jnp.where(chosen == f * per + e, route[...], 0.0), axis=0, keepdims=True)
            column[:, e * hidden : (e + 1) * hidden] = jnp.broadcast_to(weight, (hidden, tokens)).T

    def hidden_units(origin):
        step = 2 * hidden
        for n in range(per // 2):
            at = pl.ds(n * step, step)
            scaled[origin, :, at] = activations(
                normed[...], wide[0, origin, :, at], wide[1, origin, :, at], column[:, at]
            )

    def features(s):
        k = order[s][1]
        diagonal_wait(s)
        total = matmul_nt(scaled[0], block(2, 0, k)[...])
        for i in range(1, parts):
            total = total + matmul_nt(scaled[i], block(2, i, k)[...])
        part[s - base] = total.astype(jnp.bfloat16)
        device = {"fs": peer(k), "tp": t}
        remote(part.at[s - base], got.at[k - 1], send_sem.at[5], pr, device).start()

    small[0].start()
    load(0).start()
    barrier = pltpu.get_barrier_semaphore()
    for k in range(1, groups):
        pl.semaphore_signal(barrier, inc=1, device_id={"fs": peer(k), "tp": t}, device_id_type=MESH)
    for other in (tx, ty):
        pl.semaphore_signal(barrier, inc=1, device_id={"fs": f, "tp": other}, device_id_type=MESH)
    small[0].wait()
    scale[...] = jnp.broadcast_to(gain[...], (hidden, rows)).T
    load(0).wait()
    put(0, 0, block(0, t, 0))
    for k in near[1:]:
        load(k).start()
    for w in (1, 2):
        bulk(w).start()
    for copy in small[1:]:
        copy.start()
    pl.semaphore_wait(barrier, groups + 1)
    side_start(0)
    load(near[1]).wait()
    put(0, near[1], cast.at[0, near[1] - 1])
    for before, k in zip(near[1:], near[2:]):
        load(k).wait()
        put(0, k, cast.at[0, k - 1])
        z_copy(0, before).start()
    z_copy(0, near[-1]).start()

    sends = [(lag if i < 3 else lag + (i + 1) // 2, 1, k) for i, k in enumerate(near[1:])]
    sends += [(groups + 3 + i // 2, 2, k) for i, k in enumerate(near[:0:-1])]

    def step(s):
        w, k = order[s]
        if s > 0:
            if k > 0:
                z_arrival(w, k).wait_recv()
            if s == split:
                side_half(s, 0)
                forward(s - 1)
                side_half(s, half)
            else:
                side_start(s)
            if s == split + 1:
                features(s - 2)
            if s != split:
                forward(s - 1)
        for at, array, one in sends:
            if at == s:
                z_copy(array, one).start()
        if s < 2:
            put_all(s + 1)
        if s == groups:
            normalise()
            columns()
        if 3 <= s < base + 2:
            diagonal_wait(s - 3)
        if s == base:
            hidden_units(t)
        if s == base + 1:
            hidden_units(tx)
            hidden_units(ty)
        if s == base + 2:
            diagonal_wait(base - 1)
            hidden_units(td)
        if s >= base + 2 and s != split + 1:
            features(s - 2)

    def drain(end):
        forward(end - 1)
        features(end - 2)
        if order[end - 1][1] > 0:
            features(end - 1)
        else:
            diagonal_wait(end - 1)
        count = end - base
        sums = min(count, groups - 1)
        first = wide.at[:, pl.ds(0, parts - 1), pl.ds(0, width // 2)]
        second = down.at[pl.ds(0, parts - 1), pl.ds(0, count * half)]
        for i, whole in enumerate((first, second, first, second, cast, part.at[pl.ds(0, sums)])):
            remote(whole, whole, send_sem.at[i], pr, {"fs": f, "tp": tx}).wait_send()
        whole = got.at[pl.ds(0, sums)]
        remote(whole, whole, send_sem.at[5], pr, {"fs": f, "tp": tx}).wait_recv()

    for s in range(split):
        step(s)

    @pl.when(f % 2 == 1)
    def _():
        for k in evens[:-1]:
            z_arrival(2, k).wait_recv()
        drain(split)

    @pl.when(f % 2 == 0)
    def _():
        for s in range(split, len(order)):
            step(s)
        drain(len(order))


def spread(prompt, norm_gain, gate_master, up_master, down_master, group_choice, inner_choice, route_weight):
    groups, parts = lax.axis_size("fs"), lax.axis_size("tp")
    experts, rows, hidden = gate_master.shape
    per = experts // groups
    tokens, width = prompt.shape
    arrays = 3
    views = [one.reshape(groups, per, rows, hidden) for one in (gate_master, up_master, down_master)]
    dma = pltpu.SemaphoreType.DMA
    return pl.pallas_call(
        spread_body,
        in_specs=[pl.BlockSpec(memory_space=pltpu.HBM)] * 8,
        out_specs=[pl.BlockSpec(memory_space=pltpu.VMEM)] * 4,
        out_shape=[
            pltpu.VMEM((2, parts, width, per * hidden), jnp.bfloat16),
            pltpu.VMEM((parts, width, per * hidden), jnp.bfloat16),
            pltpu.VMEM((parts, tokens, per * hidden), jnp.bfloat16),
            pltpu.VMEM((groups - 1, tokens, rows), jnp.bfloat16),
        ],
        scratch_shapes=[
            pltpu.VMEM((arrays, groups, per, rows, hidden), jnp.float32),
            pltpu.VMEM((arrays, groups - 1, rows, per * hidden), jnp.bfloat16),
            pltpu.VMEM((1, rows), jnp.float32),
            pltpu.VMEM((rows, hidden), jnp.float32),
            pltpu.VMEM((tokens, width), jnp.bfloat16),
            pltpu.VMEM((tokens, width), jnp.bfloat16),
            pltpu.VMEM((1, tokens), jnp.int32),
            pltpu.VMEM((2, tokens), jnp.int32),
            pltpu.VMEM((2, tokens), jnp.float32),
            pltpu.VMEM((tokens, per * hidden), jnp.float32),
            pltpu.VMEM((groups - 1, tokens, rows), jnp.bfloat16),
            dma((groups,)),
            dma((2,)),
            dma((5,)),
            dma((6,)),
            dma((arrays, groups - 1)),
            dma((groups,)),
            dma((groups,)),
            dma((groups,)),
            dma,
        ],
        compiler_params=pltpu.CompilerParams(
            collective_id=0, has_side_effects=True, vmem_limit_bytes=32 * 1024 * 1024
        ),
        name="spread",
    )(
        norm_gain.reshape(1, rows),
        *views,
        prompt,
        group_choice.reshape(1, tokens),
        inner_choice.T,
        route_weight.T,
    )


def store_body(wide, down, gate_ref, up_ref, down_ref, token_ref, sem):
    parts, width, hold = down.shape
    hidden = FF // parts
    groups, per = lax.axis_size("fs"), hold // hidden
    rows = width // groups
    f = lax.axis_index("fs")
    _, odds, evens = block_order(groups)

    def put(k):
        at = pl.ds(pl.multiple_of(jnp.bitwise_xor(f, k) * rows, rows), rows)
        for i in range(parts):
            for e in range(per):
                pltpu.make_async_copy(
                    down.at[i, at, pl.ds(e * hidden, hidden)],
                    down_ref.at[at, pl.ds(e * FF + i * hidden, hidden)],
                    sem.at[2],
                ).start()

    def wait(count):
        done = down_ref.at[pl.ds(0, count * rows)]
        pltpu.make_async_copy(done, done, sem.at[2]).wait()

    outs = (gate_ref, up_ref)
    for w, out in enumerate(outs):
        for i in range(parts):
            for e in range(per):
                pltpu.make_async_copy(
                    wide.at[w, i, :, pl.ds(e * hidden, hidden)],
                    out.at[:, pl.ds(e * FF + i * hidden, hidden)],
                    sem.at[w],
                ).start()
    for k in odds:
        put(k)

    @pl.when(f % 2 == 0)
    def _():
        for k in evens:
            put(k)
        wait(groups)

    @pl.when(f % 2 == 1)
    def _():
        wait(len(odds))

    for w, out in enumerate(outs):
        pltpu.make_async_copy(out, out, sem.at[w]).wait()


def hold_in_vmem(*arrays):
    return [pltpu.with_memory_space_constraint(one, pltpu.VMEM) for one in arrays]


def store(wide, down):
    parts, width, hold = down.shape
    out = pltpu.HBM((width, parts * hold), down.dtype)
    vmem, hbm = pl.BlockSpec(memory_space=pltpu.VMEM), pl.BlockSpec(memory_space=pltpu.HBM)
    return pl.pallas_call(
        store_body,
        in_specs=[vmem, vmem],
        out_specs=[hbm, hbm, hbm, hbm],
        out_shape=[out, out, out, pltpu.HBM((8, 128), jnp.float32)],
        scratch_shapes=[pltpu.SemaphoreType.DMA((3,))],
        compiler_params=pltpu.CompilerParams(vmem_limit_bytes=4 * 1024 * 1024),
        name="store",
    )(*hold_in_vmem(wide, down))


def finish_body(down, scaled, got, token_ref, late, got_late, mine, part, send_sem, xr, yr, dr, pr):
    f, t = lax.axis_index("fs"), lax.axis_index("tp")
    tx, ty = jnp.bitwise_xor(t, 1), jnp.bitwise_xor(t, 2)
    parts = down.shape[0]
    rows = late.shape[2]
    half, quarter = rows // 2, rows // 4
    _, odds, evens = block_order(lax.axis_size("fs"))
    count = len(evens)

    def own(i, begin=0, size=rows):
        first = jnp.bitwise_xor(f, evens[i]) * rows + begin
        return down.at[t, pl.ds(pl.multiple_of(first, size), size)]

    pieces = [(i, c * half, half) for i in range(count) for c in range(2)]
    pieces[-1:] = [(count - 1, half, quarter), (count - 1, half + quarter, quarter)]

    def landed(j, q, which=None):
        i, begin, size = pieces[q]
        if which is not None:
            size = size // 2
            begin = begin + which * size
        return late.at[j, i, pl.ds(begin, size)]

    def x_copy(q):
        source = own(*pieces[q])
        return remote(source, landed(0, q), send_sem.at[0], xr.at[q], {"fs": f, "tp": tx})

    def y_copy(q):
        source = own(*pieces[q])
        return remote(source, landed(1, q), send_sem.at[1], yr.at[q], {"fs": f, "tp": ty})

    def to_y(q):
        source, target = landed(0, q, 0), landed(2, q, 0)
        return remote(source, target, send_sem.at[1], dr.at[q], {"fs": f, "tp": ty})

    def to_x(q):
        source, target = landed(1, q, 1), landed(2, q, 1)
        return remote(source, target, send_sem.at[0], dr.at[q], {"fs": f, "tp": tx})

    def side_start(q):
        x_copy(q).start()
        y_copy(q).start()

    def forward(q):
        x_copy(q).wait_recv()
        to_y(q).start()
        y_copy(q).wait_recv()
        to_x(q).start()

    def straight(i):
        total = matmul_nt(scaled[t], own(i)[...])
        for j in (1, 2):
            total = total + matmul_nt(scaled[jnp.bitwise_xor(t, j)], late[j - 1, i])
        return total

    def diagonal(i):
        for q in [q for q, piece in enumerate(pieces) if piece[0] == i]:
            one = landed(2, q)
            remote(one, one, send_sem.at[0], dr.at[q], {"fs": f, "tp": tx}).wait_recv()
        return matmul_nt(scaled[jnp.bitwise_xor(t, 3)], late[2, i])

    def features(i):
        mine[...] = straight(i)
        part[i] = (mine[...] + diagonal(i)).astype(jnp.bfloat16)
        device = {"fs": jnp.bitwise_xor(f, evens[i]), "tp": t}
        remote(part.at[i], got_late.at[i], send_sem.at[2], pr, device).start()

    def collected(total, chosen):
        for k in chosen:
            total = total + got[k - 1].astype(jnp.float32)
        return total

    def run():
        total, sent = len(pieces), 0
        for q in range(total):
            goal = 4 if q == 0 else 5 + q // 2
            if q >= 2 * count - 2:
                goal = total
            while sent < min(goal, total):
                side_start(sent)
                sent += 1
            if q >= 4 and q % 2 == 0 and q < 2 * count - 1:
                features(q // 2 - 2)
            forward(q)
            if q == 2 * count - 2:
                features(count - 2)
        mine[...] = collected(straight(count - 1), odds)
        mine[...] += diagonal(count - 1)
        sides = late.at[:, :, pl.ds(0, half)]
        for i, whole in enumerate((sides, sides, part)):
            remote(whole, whole, send_sem.at[i], pr, {"fs": f, "tp": tx}).wait_send()
        remote(got_late, got_late, send_sem.at[2], pr, {"fs": f, "tp": tx}).wait_recv()

    @pl.when(f % 2 == 1)
    def _():
        barrier = pltpu.get_barrier_semaphore()
        others = [{"fs": jnp.bitwise_xor(f, k), "tp": t} for k in evens[:-1]]
        others += [{"fs": f, "tp": tx}, {"fs": f, "tp": ty}]
        for other in others:
            pl.semaphore_signal(barrier, inc=1, device_id=other, device_id_type=MESH)
        pl.semaphore_wait(barrier, len(others))
        run()

    @pl.when(f % 2 == 0)
    def _():
        at = pl.ds(pl.multiple_of(f * rows, rows), rows)
        total = matmul_nt(scaled[0], down[0, at, :])
        for i in range(1, parts):
            total = total + matmul_nt(scaled[i], down[i, at, :])
        mine[...] = collected(total, odds + evens[:-1])


def finish(down, scaled, got, token, groups):
    parts, width, hold = down.shape
    tokens, rows, count = scaled.shape[1], width // groups, groups // 2
    vmem, hbm = pl.BlockSpec(memory_space=pltpu.VMEM), pl.BlockSpec(memory_space=pltpu.HBM)
    dma = pltpu.SemaphoreType.DMA
    return pl.pallas_call(
        finish_body,
        in_specs=[vmem, vmem, vmem, hbm],
        out_specs=[vmem, vmem, vmem],
        out_shape=[
            pltpu.VMEM((parts - 1, count, rows, hold), down.dtype),
            pltpu.VMEM((count - 1, tokens, rows), jnp.bfloat16),
            pltpu.VMEM((tokens, rows), jnp.float32),
        ],
        scratch_shapes=[
            pltpu.VMEM((count - 1, tokens, rows), jnp.bfloat16),
            dma((3,)),
            dma((2 * count + 1,)),
            dma((2 * count + 1,)),
            dma((2 * count + 1,)),
            dma,
        ],
        compiler_params=pltpu.CompilerParams(
            collective_id=1, has_side_effects=True, vmem_limit_bytes=4 * 1024 * 1024
        ),
        name="finish",
    )(*hold_in_vmem(down, scaled, got), pltpu.with_memory_space_constraint(token, pltpu.HBM))


def serve_body(down, late, got_late, mine, down_in, down_ref, mixed_ref, mixed, sem):
    parts, width, hold = down.shape
    hidden, rows = FF // parts, late.shape[2]
    f, t = lax.axis_index("fs"), lax.axis_index("tp")
    _, _, evens = block_order(width // rows)
    count = len(evens)

    def put(i):
        at = pl.ds(pl.multiple_of(jnp.bitwise_xor(f, evens[i]) * rows, rows), rows)
        for j in range(parts):
            origin = jnp.bitwise_xor(t, j)
            source = late.at[j - 1, i] if j > 0 else down.at[t, at]
            for e in range(hold // hidden):
                begin = pl.multiple_of(e * FF + origin * hidden, hidden)
                pltpu.make_async_copy(
                    source.at[:, pl.ds(e * hidden, hidden)], down_ref.at[at, pl.ds(begin, hidden)], sem.at[0]
                ).start()

    def finish_mixed(total):
        mixed[...] = (total * FF ** (-0.5)).astype(jnp.bfloat16)
        final = pltpu.make_async_copy(mixed, mixed_ref, sem.at[1])
        final.start()
        return final

    @pl.when(f % 2 == 1)
    def _():
        for i in range(count):
            put(i)
        total = mine[...]
        for i in range(count - 1):
            total = total + got_late[i].astype(jnp.float32)
        final = finish_mixed(total)
        done = down_ref.at[pl.ds(0, count * rows)]
        pltpu.make_async_copy(done, done, sem.at[0]).wait()
        final.wait()

    @pl.when(f % 2 == 0)
    def _():
        finish_mixed(mine[...]).wait()


def serve(down, late, got_late, mine, down_out):
    tokens, rows = mine.shape
    vmem, hbm = pl.BlockSpec(memory_space=pltpu.VMEM), pl.BlockSpec(memory_space=pltpu.HBM)
    return pl.pallas_call(
        serve_body,
        in_specs=[vmem] * 4 + [hbm],
        out_specs=[hbm, hbm],
        out_shape=[pltpu.HBM(down_out.shape, down_out.dtype), pltpu.HBM((tokens, rows), jnp.bfloat16)],
        input_output_aliases={4: 0},
        scratch_shapes=[pltpu.VMEM((tokens, rows), jnp.bfloat16), pltpu.SemaphoreType.DMA((2,))],
        compiler_params=pltpu.CompilerParams(vmem_limit_bytes=4 * 1024 * 1024),
        name="serve",
    )(*hold_in_vmem(down, late, got_late, mine), pltpu.with_memory_space_constraint(down_out, pltpu.HBM))


def direct_shards(
    prompt, norm_gain, gate_master, up_master, down_master, group_choice, inner_choice, route_weight
):
    groups = lax.axis_size("fs")
    wide, down, scaled, got = spread(
        prompt, norm_gain, gate_master, up_master, down_master, group_choice, inner_choice, route_weight
    )
    gate_local, up_local, down_some, token = store(wide, down)
    late, got_late, mine = finish(down, scaled, got, token, groups)
    down_local, mixed = serve(down, late, got_late, mine, down_some)
    return (gate_local, up_local, down_local, mixed)


def fits_direct(mesh):
    groups, parts = mesh.shape["fs"], mesh.shape["tp"]
    whole_experts = (GROUPS * EPG) % groups == 0 and (GROUPS * EPG // groups) % 2 == 0
    return parts == 4 and groups >= 4 and groups & (groups - 1) == 0 and whole_experts and FF // parts % 128 == 0


def solution(mesh):
    in_specs = (
        P("tp", None),
        P("fs"),
        P(None, "fs", "tp"),
        P(None, "fs", "tp"),
        P(None, "fs", "tp"),
        P("tp"),
        P("tp", None),
        P("tp", None),
    )
    out_specs = (P(None, "fs"), P(None, "fs"), P(None, "fs"), P("tp", "fs"))
    body = direct_shards if fits_direct(mesh) else shards
    return jax.shard_map(body, mesh=mesh, in_specs=in_specs, out_specs=out_specs, check_vma=False)
```

```python
import jax
import jax.numpy as jnp
from jax import lax
from jax.experimental import pallas as pl
from jax.experimental.pallas import tpu as pltpu
from jax.sharding import PartitionSpec as P

MESH = pl.DeviceIdType.MESH
FF = 512
GROUPS = 4
EPG = 8


def flatten_rows(piece):
    count, experts, rows, hidden = piece.shape
    return piece.transpose(0, 2, 1, 3).reshape(count, rows, experts * hidden)


def restore_rows(gathered, rows):
    parts = lax.axis_size("tp")
    count, total, width = gathered.shape
    blocks = total // (parts * rows)
    ordered = gathered.reshape(count, parts, blocks, rows, width).transpose(0, 2, 1, 3, 4)
    return ordered.reshape(count, total, width)


def activations(normed, gate_local, up_local, column_weight):
    width = normed.shape[1]
    gate_act = jnp.dot(normed, gate_local, preferred_element_type=jnp.float32) * width ** (-0.5)
    up_act = jnp.dot(normed, up_local, preferred_element_type=jnp.float32) * width ** (-0.5)
    return (column_weight * jax.nn.silu(gate_act) * up_act).astype(jnp.bfloat16)


def route_columns(weight, columns, experts):
    first = lax.axis_index("fs") * columns
    owner = (first + jnp.arange(columns, dtype=jnp.int32)) // FF
    onehot = (owner[None, :] == jnp.arange(experts, dtype=jnp.int32)[:, None]).astype(jnp.float32)
    return jnp.dot(weight, onehot, precision=lax.Precision.HIGHEST)


def shards(
    prompt, norm_gain, gate_master, up_master, down_master, group_choice, inner_choice, route_weight
):
    experts = GROUPS * EPG
    scale = norm_gain[None, :, None]
    gate_cast = (gate_master * scale).astype(jnp.bfloat16)
    up_cast = (up_master * scale).astype(jnp.bfloat16)
    down_cast = down_master.astype(jnp.bfloat16)
    rows = gate_master.shape[1] // lax.axis_size("tp")
    values = prompt.astype(jnp.float32)
    normed = (values * lax.rsqrt(jnp.mean(values * values, axis=1, keepdims=True) + 1e-06)).astype(
        jnp.bfloat16
    )
    chosen = group_choice[:, None] * EPG + inner_choice
    member = (chosen[:, :, None] == jnp.arange(experts, dtype=jnp.int32)[None, None, :]).astype(
        jnp.float32
    )
    weight = jnp.sum(member * route_weight[:, :, None], axis=1)
    stacked = jnp.stack([gate_cast, up_cast, down_cast])
    widened = lax.all_to_all(stacked, "tp", split_axis=2, concat_axis=3, tiled=True)
    moved = lax.all_to_all(flatten_rows(widened), "fs", split_axis=2, concat_axis=1, tiled=True)
    served = restore_rows(lax.all_gather(moved, "tp", axis=1, tiled=True), rows)
    gate_local, up_local, down_local = (served[0], served[1], served[2])
    column_weight = route_columns(weight, gate_local.shape[1], experts)
    scaled = activations(normed, gate_local, up_local, column_weight)
    summed = lax.psum_scatter(
        lax.dot_general(
            down_local, scaled, (((1,), (1,)), ((), ())), preferred_element_type=jnp.float32
        ),
        "fs",
        scatter_dimension=0,
        tiled=True,
    )
    mixed = (summed * FF ** (-0.5)).T.astype(jnp.bfloat16)
    return (gate_local, up_local, down_local, mixed)


def remote(source, target, send, recv, device):
    return pltpu.make_async_remote_copy(
        src_ref=source,
        dst_ref=target,
        send_sem=send,
        recv_sem=recv,
        device_id=device,
        device_id_type=MESH,
    )


def block_order(groups):
    near = [2 * (i ^ (i >> 1)) + c for i in range(groups // 2) for c in range(2)]
    last = near[::-1]
    return near, [k for k in last if k % 2 == 1], [k for k in last if k % 2 == 0]


def matmul_nt(left, right):
    return lax.dot_general(left, right, (((1,), (1,)), ((), ())), preferred_element_type=jnp.float32)


def spread_body(
    gain_ref,
    gate_ref,
    up_ref,
    down_ref,
    prompt_ref,
    group_ref,
    inner_ref,
    route_ref,
    wide,
    down,
    scaled,
    got,
    raw,
    cast,
    gain,
    scale,
    prompt,
    normed,
    group,
    inner,
    route,
    column,
    part,
    load_sem,
    bulk_sem,
    small_sem,
    send_sem,
    zr,
    xr,
    yr,
    dr,
    pr,
    column_in,
):
    f, t = lax.axis_index("fs"), lax.axis_index("tp")
    tx, ty, td = jnp.bitwise_xor(t, 1), jnp.bitwise_xor(t, 2), jnp.bitwise_xor(t, 3)
    arrays, groups, per, rows, hidden = raw.shape
    parts, width = down.shape[:2]
    tokens = prompt.shape[0]
    half = rows // 2
    masters = (gate_ref, up_ref, down_ref)
    near, odds, evens = block_order(groups)
    order = [(w, k) for w in range(2) for k in near] + [(2, k) for k in odds + evens]
    base, split, lag = 2 * groups, 2 * groups + len(odds), groups // 2

    def peer(k):
        return jnp.bitwise_xor(f, k)

    def load(k):
        return pltpu.make_async_copy(gate_ref.at[peer(k)], raw.at[0, peer(k)], load_sem.at[k])

    def bulk(w):
        return pltpu.make_async_copy(masters[w], raw.at[w], bulk_sem.at[w - 1])

    small = [
        pltpu.make_async_copy(source, target, small_sem.at[i])
        for i, (source, target) in enumerate(
            (
                (gain_ref, gain),
                (prompt_ref, prompt),
                (group_ref, group),
                (inner_ref, inner),
                (route_ref, route),
            )
        )
    ]

    def block(w, origin, k, begin=0, count=rows):
        at = pl.ds(pl.multiple_of(peer(k) * rows + begin, count), count)
        return wide.at[w, origin, at] if w < 2 else down.at[origin, at]

    def z_copy(w, k):
        device = {"fs": peer(k), "tp": t}
        return remote(cast.at[w, k - 1], block(w, t, 0), send_sem.at[4], zr.at[w, k - 1], device)

    def z_arrival(w, k):
        device = {"fs": peer(k), "tp": t}
        return remote(cast.at[w, k - 1], block(w, t, k), send_sem.at[4], zr.at[w, k - 1], device)

    def x_copy(s, origin):
        one = block(order[s][0], origin, order[s][1])
        return remote(one, one, send_sem.at[s // base], xr.at[s % groups], {"fs": f, "tp": tx})

    def y_copy(s, origin):
        one = block(order[s][0], origin, order[s][1])
        return remote(one, one, send_sem.at[2 + s // base], yr.at[s % groups], {"fs": f, "tp": ty})

    def to_x(s):
        one = block(order[s][0], ty, order[s][1], half, half)
        return remote(one, one, send_sem.at[s // base], dr.at[s % groups], {"fs": f, "tp": tx})

    def to_y(s):
        one = block(order[s][0], tx, order[s][1], 0, half)
        return remote(one, one, send_sem.at[2 + s // base], dr.at[s % groups], {"fs": f, "tp": ty})

    def diagonal_wait(s):
        one = block(order[s][0], td, order[s][1])
        remote(one, one, send_sem.at[0], dr.at[s % groups], {"fs": f, "tp": tx}).wait_recv()

    def side_start(s):
        x_copy(s, t).start()
        y_copy(s, t).start()

    def side_half(s, begin):
        one = block(order[s][0], t, order[s][1], begin, half)
        remote(one, one, send_sem.at[s // base], xr.at[s % groups], {"fs": f, "tp": tx}).start()
        remote(one, one, send_sem.at[2 + s // base], yr.at[s % groups], {"fs": f, "tp": ty}).start()

    def forward(s):
        x_copy(s, tx).wait_recv()
        to_y(s).start()
        y_copy(s, ty).wait_recv()
        to_x(s).start()

    def put(w, k, target):
        for e in range(per):
            value = raw[w, peer(k), e]
            if w < 2:
                value = value * scale[...]
            target[:, e * hidden : (e + 1) * hidden] = value.astype(jnp.bfloat16)

    def put_all(w):
        bulk(w).wait()
        put(w, 0, block(w, t, 0))

        def one(k, carry):
            put(w, k, cast.at[w, k - 1])
            return carry

        lax.fori_loop(1, groups, one, 0)

    def normalise():
        small[1].wait()
        values = prompt[...].astype(jnp.float32)
        mean = jnp.mean(values * values, axis=1, keepdims=True)
        normed[...] = (values * lax.rsqrt(mean + 1e-06)).astype(jnp.bfloat16)

    def columns():
        for i in range(2, 5):
            small[i].wait()
        chosen = group[...] * EPG + inner[...]
        for e in range(per):
            weight = jnp.sum(jnp.where(chosen == f * per + e, route[...], 0.0), axis=0, keepdims=True)
            column[:, e * hidden : (e + 1) * hidden] = jnp.broadcast_to(weight, (hidden, tokens)).T

    def hidden_units(origin):
        step = 2 * hidden
        for n in range(per // 2):
            at = pl.ds(n * step, step)
            scaled[origin, :, at] = activations(
                normed[...], wide[0, origin, :, at], wide[1, origin, :, at], column[:, at]
            )

    def features(s):
        k = order[s][1]
        diagonal_wait(s)
        total = matmul_nt(scaled[0], block(2, 0, k)[...])
        for i in range(1, parts):
            total = total + matmul_nt(scaled[i], block(2, i, k)[...])
        part[s - base] = total.astype(jnp.bfloat16)
        device = {"fs": peer(k), "tp": t}
        remote(part.at[s - base], got.at[k - 1], send_sem.at[5], pr, device).start()

    small[0].start()
    load(0).start()
    barrier = pltpu.get_barrier_semaphore()

    def greet(chosen):
        for k in chosen:
            device = {"fs": peer(k), "tp": t}
            pl.semaphore_signal(barrier, inc=1, device_id=device, device_id_type=MESH)

    @pl.when(f % 2 == 0)
    def _():
        greet([1] + list(range(2, groups, 2)))

    @pl.when(f % 2 == 1)
    def _():
        greet(range(1, groups, 2))

    for other in (tx, ty):
        pl.semaphore_signal(barrier, inc=1, device_id={"fs": f, "tp": other}, device_id_type=MESH)
    small[0].wait()
    scale[...] = jnp.broadcast_to(gain[...], (hidden, rows)).T
    load(0).wait()
    put(0, 0, block(0, t, 0))
    for k in near[1:]:
        load(k).start()
    for w in (1, 2):
        bulk(w).start()
    for copy in small[1:]:
        copy.start()
    pl.semaphore_wait(barrier, 3 + (groups - 2) * (1 - f % 2))
    side_start(0)
    load(near[1]).wait()
    put(0, near[1], cast.at[0, near[1] - 1])

    @pl.when(f % 2 == 0)
    def _():
        pl.semaphore_signal(column_in, inc=1, device_id={"fs": peer(1), "tp": t}, device_id_type=MESH)

    @pl.when(f % 2 == 1)
    def _():
        pl.semaphore_wait(column_in, 1)

    for before, k in zip(near[1:], near[2:]):
        load(k).wait()
        put(0, k, cast.at[0, k - 1])
        z_copy(0, before).start()
    z_copy(0, near[-1]).start()

    sends = [(lag if i < 3 else lag + (i + 1) // 2, 1, k) for i, k in enumerate(near[1:])]
    sends += [(groups + 3 + i // 2, 2, k) for i, k in enumerate(near[:0:-1])]

    def step(s):
        w, k = order[s]
        if s > 0:
            if k > 0:
                z_arrival(w, k).wait_recv()
            if s == split:
                side_half(s, 0)
                forward(s - 1)
                side_half(s, half)
            else:
                side_start(s)
            if s == split + 1:
                features(s - 2)
            if s != split:
                forward(s - 1)
        for at, array, one in sends:
            if at == s:
                z_copy(array, one).start()
        if s < 2:
            put_all(s + 1)
        if s == groups:
            normalise()
            columns()
        if 3 <= s < base + 2:
            diagonal_wait(s - 3)
        if s == base:
            hidden_units(t)
        if s == base + 1:
            hidden_units(tx)
            hidden_units(ty)
        if s == base + 2:
            diagonal_wait(base - 1)
            hidden_units(td)
        if s >= base + 2 and s != split + 1:
            features(s - 2)

    def drain(end):
        forward(end - 1)
        features(end - 2)
        if order[end - 1][1] > 0:
            features(end - 1)
        else:
            diagonal_wait(end - 1)
        count = end - base
        sums = min(count, groups - 1)
        first = wide.at[:, pl.ds(0, parts - 1), pl.ds(0, width // 2)]
        second = down.at[pl.ds(0, parts - 1), pl.ds(0, count * half)]
        for i, whole in enumerate((first, second, first, second, cast, part.at[pl.ds(0, sums)])):
            remote(whole, whole, send_sem.at[i], pr, {"fs": f, "tp": tx}).wait_send()
        whole = got.at[pl.ds(0, sums)]
        remote(whole, whole, send_sem.at[5], pr, {"fs": f, "tp": tx}).wait_recv()

    for s in range(split):
        step(s)

    @pl.when(f % 2 == 1)
    def _():
        for k in evens[:-1]:
            z_arrival(2, k).wait_recv()
        drain(split)

    @pl.when(f % 2 == 0)
    def _():
        for s in range(split, len(order)):
            step(s)
        drain(len(order))


def spread(prompt, norm_gain, gate_master, up_master, down_master, group_choice, inner_choice, route_weight):
    groups, parts = lax.axis_size("fs"), lax.axis_size("tp")
    experts, rows, hidden = gate_master.shape
    per = experts // groups
    tokens, width = prompt.shape
    arrays = 3
    views = [one.reshape(groups, per, rows, hidden) for one in (gate_master, up_master, down_master)]
    dma = pltpu.SemaphoreType.DMA
    return pl.pallas_call(
        spread_body,
        in_specs=[pl.BlockSpec(memory_space=pltpu.HBM)] * 8,
        out_specs=[pl.BlockSpec(memory_space=pltpu.VMEM)] * 4,
        out_shape=[
            pltpu.VMEM((2, parts, width, per * hidden), jnp.bfloat16),
            pltpu.VMEM((parts, width, per * hidden), jnp.bfloat16),
            pltpu.VMEM((parts, tokens, per * hidden), jnp.bfloat16),
            pltpu.VMEM((groups - 1, tokens, rows), jnp.bfloat16),
        ],
        scratch_shapes=[
            pltpu.VMEM((arrays, groups, per, rows, hidden), jnp.float32),
            pltpu.VMEM((arrays, groups - 1, rows, per * hidden), jnp.bfloat16),
            pltpu.VMEM((1, rows), jnp.float32),
            pltpu.VMEM((rows, hidden), jnp.float32),
            pltpu.VMEM((tokens, width), jnp.bfloat16),
            pltpu.VMEM((tokens, width), jnp.bfloat16),
            pltpu.VMEM((1, tokens), jnp.int32),
            pltpu.VMEM((2, tokens), jnp.int32),
            pltpu.VMEM((2, tokens), jnp.float32),
            pltpu.VMEM((tokens, per * hidden), jnp.float32),
            pltpu.VMEM((groups - 1, tokens, rows), jnp.bfloat16),
            dma((groups,)),
            dma((2,)),
            dma((5,)),
            dma((6,)),
            dma((arrays, groups - 1)),
            dma((groups,)),
            dma((groups,)),
            dma((groups,)),
            dma,
            pltpu.SemaphoreType.REGULAR,
        ],
        compiler_params=pltpu.CompilerParams(
            collective_id=0, has_side_effects=True, vmem_limit_bytes=32 * 1024 * 1024
        ),
        name="spread",
    )(
        norm_gain.reshape(1, rows),
        *views,
        prompt,
        group_choice.reshape(1, tokens),
        inner_choice.T,
        route_weight.T,
    )


def store_body(wide, down, gate_ref, up_ref, down_ref, token_ref, sem):
    parts, width, hold = down.shape
    hidden = FF // parts
    groups, per = lax.axis_size("fs"), hold // hidden
    rows = width // groups
    f = lax.axis_index("fs")
    _, odds, evens = block_order(groups)

    def put(k):
        at = pl.ds(pl.multiple_of(jnp.bitwise_xor(f, k) * rows, rows), rows)
        for i in range(parts):
            for e in range(per):
                pltpu.make_async_copy(
                    down.at[i, at, pl.ds(e * hidden, hidden)],
                    down_ref.at[at, pl.ds(e * FF + i * hidden, hidden)],
                    sem.at[2],
                ).start()

    def wait(count):
        done = down_ref.at[pl.ds(0, count * rows)]
        pltpu.make_async_copy(done, done, sem.at[2]).wait()

    outs = (gate_ref, up_ref)
    for w, out in enumerate(outs):
        for i in range(parts):
            for e in range(per):
                pltpu.make_async_copy(
                    wide.at[w, i, :, pl.ds(e * hidden, hidden)],
                    out.at[:, pl.ds(e * FF + i * hidden, hidden)],
                    sem.at[w],
                ).start()
    for k in odds:
        put(k)

    @pl.when(f % 2 == 0)
    def _():
        for k in evens:
            put(k)
        wait(groups)

    @pl.when(f % 2 == 1)
    def _():
        wait(len(odds))

    for w, out in enumerate(outs):
        pltpu.make_async_copy(out, out, sem.at[w]).wait()


def hold_in_vmem(*arrays):
    return [pltpu.with_memory_space_constraint(one, pltpu.VMEM) for one in arrays]


def store(wide, down):
    parts, width, hold = down.shape
    out = pltpu.HBM((width, parts * hold), down.dtype)
    vmem, hbm = pl.BlockSpec(memory_space=pltpu.VMEM), pl.BlockSpec(memory_space=pltpu.HBM)
    return pl.pallas_call(
        store_body,
        in_specs=[vmem, vmem],
        out_specs=[hbm, hbm, hbm, hbm],
        out_shape=[out, out, out, pltpu.HBM((8, 128), jnp.float32)],
        scratch_shapes=[pltpu.SemaphoreType.DMA((3,))],
        compiler_params=pltpu.CompilerParams(vmem_limit_bytes=4 * 1024 * 1024),
        name="store",
    )(*hold_in_vmem(wide, down))


def finish_body(down, scaled, got, token_ref, late, got_late, mine, part, send_sem, xr, yr, dr, pr):
    f, t = lax.axis_index("fs"), lax.axis_index("tp")
    tx, ty = jnp.bitwise_xor(t, 1), jnp.bitwise_xor(t, 2)
    parts = down.shape[0]
    rows = late.shape[2]
    half, quarter = rows // 2, rows // 4
    _, odds, evens = block_order(lax.axis_size("fs"))
    count = len(evens)

    def own(i, begin=0, size=rows):
        first = jnp.bitwise_xor(f, evens[i]) * rows + begin
        return down.at[t, pl.ds(pl.multiple_of(first, size), size)]

    pieces = [(i, c * half, half) for i in range(count) for c in range(2)]
    pieces[-1:] = [(count - 1, half, quarter), (count - 1, half + quarter, quarter)]

    def landed(j, q, which=None):
        i, begin, size = pieces[q]
        if which is not None:
            size = size // 2
            begin = begin + which * size
        return late.at[j, i, pl.ds(begin, size)]

    def x_copy(q):
        source = own(*pieces[q])
        return remote(source, landed(0, q), send_sem.at[0], xr.at[q], {"fs": f, "tp": tx})

    def y_copy(q):
        source = own(*pieces[q])
        return remote(source, landed(1, q), send_sem.at[1], yr.at[q], {"fs": f, "tp": ty})

    def to_y(q):
        source, target = landed(0, q, 0), landed(2, q, 0)
        return remote(source, target, send_sem.at[1], dr.at[q], {"fs": f, "tp": ty})

    def to_x(q):
        source, target = landed(1, q, 1), landed(2, q, 1)
        return remote(source, target, send_sem.at[0], dr.at[q], {"fs": f, "tp": tx})

    def side_start(q):
        x_copy(q).start()
        y_copy(q).start()

    def forward(q):
        x_copy(q).wait_recv()
        to_y(q).start()
        y_copy(q).wait_recv()
        to_x(q).start()

    def straight(i):
        total = matmul_nt(scaled[t], own(i)[...])
        for j in (1, 2):
            total = total + matmul_nt(scaled[jnp.bitwise_xor(t, j)], late[j - 1, i])
        return total

    def diagonal(i):
        for q in [q for q, piece in enumerate(pieces) if piece[0] == i]:
            one = landed(2, q)
            remote(one, one, send_sem.at[0], dr.at[q], {"fs": f, "tp": tx}).wait_recv()
        return matmul_nt(scaled[jnp.bitwise_xor(t, 3)], late[2, i])

    def features(i):
        mine[...] = straight(i)
        part[i] = (mine[...] + diagonal(i)).astype(jnp.bfloat16)
        device = {"fs": jnp.bitwise_xor(f, evens[i]), "tp": t}
        remote(part.at[i], got_late.at[i], send_sem.at[2], pr, device).start()

    def collected(total, chosen):
        for k in chosen:
            total = total + got[k - 1].astype(jnp.float32)
        return total

    def run():
        total, sent = len(pieces), 0
        for q in range(total):
            goal = 4 if q == 0 else 5 + q // 2
            if q >= 2 * count - 2:
                goal = total
            while sent < min(goal, total):
                side_start(sent)
                sent += 1
            if q >= 4 and q % 2 == 0 and q < 2 * count - 1:
                features(q // 2 - 2)
            forward(q)
            if q == 2 * count - 2:
                features(count - 2)
        mine[...] = collected(straight(count - 1), odds)
        mine[...] += diagonal(count - 1)
        sides = late.at[:, :, pl.ds(0, half)]
        for i, whole in enumerate((sides, sides, part)):
            remote(whole, whole, send_sem.at[i], pr, {"fs": f, "tp": tx}).wait_send()
        remote(got_late, got_late, send_sem.at[2], pr, {"fs": f, "tp": tx}).wait_recv()

    @pl.when(f % 2 == 1)
    def _():
        barrier = pltpu.get_barrier_semaphore()
        others = [{"fs": jnp.bitwise_xor(f, k), "tp": t} for k in evens[:-1]]
        others += [{"fs": f, "tp": tx}, {"fs": f, "tp": ty}]
        for other in others:
            pl.semaphore_signal(barrier, inc=1, device_id=other, device_id_type=MESH)
        pl.semaphore_wait(barrier, len(others))
        run()

    @pl.when(f % 2 == 0)
    def _():
        at = pl.ds(pl.multiple_of(f * rows, rows), rows)
        total = matmul_nt(scaled[0], down[0, at, :])
        for i in range(1, parts):
            total = total + matmul_nt(scaled[i], down[i, at, :])
        mine[...] = collected(total, odds + evens[:-1])


def finish(down, scaled, got, token, groups):
    parts, width, hold = down.shape
    tokens, rows, count = scaled.shape[1], width // groups, groups // 2
    vmem, hbm = pl.BlockSpec(memory_space=pltpu.VMEM), pl.BlockSpec(memory_space=pltpu.HBM)
    dma = pltpu.SemaphoreType.DMA
    return pl.pallas_call(
        finish_body,
        in_specs=[vmem, vmem, vmem, hbm],
        out_specs=[vmem, vmem, vmem],
        out_shape=[
            pltpu.VMEM((parts - 1, count, rows, hold), down.dtype),
            pltpu.VMEM((count - 1, tokens, rows), jnp.bfloat16),
            pltpu.VMEM((tokens, rows), jnp.float32),
        ],
        scratch_shapes=[
            pltpu.VMEM((count - 1, tokens, rows), jnp.bfloat16),
            dma((3,)),
            dma((2 * count + 1,)),
            dma((2 * count + 1,)),
            dma((2 * count + 1,)),
            dma,
        ],
        compiler_params=pltpu.CompilerParams(
            collective_id=1, has_side_effects=True, vmem_limit_bytes=4 * 1024 * 1024
        ),
        name="finish",
    )(*hold_in_vmem(down, scaled, got), pltpu.with_memory_space_constraint(token, pltpu.HBM))


def serve_body(down, late, got_late, mine, down_in, down_ref, mixed_ref, mixed, sem):
    parts, width, hold = down.shape
    hidden, rows = FF // parts, late.shape[2]
    f, t = lax.axis_index("fs"), lax.axis_index("tp")
    _, _, evens = block_order(width // rows)
    count = len(evens)

    def put(i):
        at = pl.ds(pl.multiple_of(jnp.bitwise_xor(f, evens[i]) * rows, rows), rows)
        for j in range(parts):
            origin = jnp.bitwise_xor(t, j)
            source = late.at[j - 1, i] if j > 0 else down.at[t, at]
            for e in range(hold // hidden):
                begin = pl.multiple_of(e * FF + origin * hidden, hidden)
                pltpu.make_async_copy(
                    source.at[:, pl.ds(e * hidden, hidden)], down_ref.at[at, pl.ds(begin, hidden)], sem.at[0]
                ).start()

    def finish_mixed(total):
        mixed[...] = (total * FF ** (-0.5)).astype(jnp.bfloat16)
        final = pltpu.make_async_copy(mixed, mixed_ref, sem.at[1])
        final.start()
        return final

    @pl.when(f % 2 == 1)
    def _():
        for i in range(count):
            put(i)
        total = mine[...]
        for i in range(count - 1):
            total = total + got_late[i].astype(jnp.float32)
        final = finish_mixed(total)
        done = down_ref.at[pl.ds(0, count * rows)]
        pltpu.make_async_copy(done, done, sem.at[0]).wait()
        final.wait()

    @pl.when(f % 2 == 0)
    def _():
        finish_mixed(mine[...]).wait()


def serve(down, late, got_late, mine, down_out):
    tokens, rows = mine.shape
    vmem, hbm = pl.BlockSpec(memory_space=pltpu.VMEM), pl.BlockSpec(memory_space=pltpu.HBM)
    return pl.pallas_call(
        serve_body,
        in_specs=[vmem] * 4 + [hbm],
        out_specs=[hbm, hbm],
        out_shape=[pltpu.HBM(down_out.shape, down_out.dtype), pltpu.HBM((tokens, rows), jnp.bfloat16)],
        input_output_aliases={4: 0},
        scratch_shapes=[pltpu.VMEM((tokens, rows), jnp.bfloat16), pltpu.SemaphoreType.DMA((2,))],
        compiler_params=pltpu.CompilerParams(vmem_limit_bytes=4 * 1024 * 1024),
        name="serve",
    )(*hold_in_vmem(down, late, got_late, mine), pltpu.with_memory_space_constraint(down_out, pltpu.HBM))


def direct_shards(
    prompt, norm_gain, gate_master, up_master, down_master, group_choice, inner_choice, route_weight
):
    groups = lax.axis_size("fs")
    wide, down, scaled, got = spread(
        prompt, norm_gain, gate_master, up_master, down_master, group_choice, inner_choice, route_weight
    )
    gate_local, up_local, down_some, token = store(wide, down)
    late, got_late, mine = finish(down, scaled, got, token, groups)
    down_local, mixed = serve(down, late, got_late, mine, down_some)
    return (gate_local, up_local, down_local, mixed)


def fits_direct(mesh):
    groups, parts = mesh.shape["fs"], mesh.shape["tp"]
    whole_experts = (GROUPS * EPG) % groups == 0 and (GROUPS * EPG // groups) % 2 == 0
    return parts == 4 and groups >= 4 and groups & (groups - 1) == 0 and whole_experts and FF // parts % 128 == 0


def solution(mesh):
    in_specs = (
        P("tp", None),
        P("fs"),
        P(None, "fs", "tp"),
        P(None, "fs", "tp"),
        P(None, "fs", "tp"),
        P("tp"),
        P("tp", None),
        P("tp", None),
    )
    out_specs = (P(None, "fs"), P(None, "fs"), P(None, "fs"), P("tp", "fs"))
    body = direct_shards if fits_direct(mesh) else shards
    return jax.shard_map(body, mesh=mesh, in_specs=in_specs, out_specs=out_specs, check_vma=False)
```

```python
import jax
import jax.numpy as jnp
from jax import lax
from jax.experimental import pallas as pl
from jax.experimental.pallas import tpu as pltpu
from jax.sharding import PartitionSpec as P

MESH = pl.DeviceIdType.MESH
FF = 512
GROUPS = 4
EPG = 8


def flatten_rows(piece):
    count, experts, rows, hidden = piece.shape
    return piece.transpose(0, 2, 1, 3).reshape(count, rows, experts * hidden)


def restore_rows(gathered, rows):
    parts = lax.axis_size("tp")
    count, total, width = gathered.shape
    blocks = total // (parts * rows)
    ordered = gathered.reshape(count, parts, blocks, rows, width).transpose(0, 2, 1, 3, 4)
    return ordered.reshape(count, total, width)


def activations(normed, gate_local, up_local, column_weight):
    width = normed.shape[1]
    gate_act = jnp.dot(normed, gate_local, preferred_element_type=jnp.float32) * width ** (-0.5)
    up_act = jnp.dot(normed, up_local, preferred_element_type=jnp.float32) * width ** (-0.5)
    return (column_weight * jax.nn.silu(gate_act) * up_act).astype(jnp.bfloat16)


def route_columns(weight, columns, experts):
    first = lax.axis_index("fs") * columns
    owner = (first + jnp.arange(columns, dtype=jnp.int32)) // FF
    onehot = (owner[None, :] == jnp.arange(experts, dtype=jnp.int32)[:, None]).astype(jnp.float32)
    return jnp.dot(weight, onehot, precision=lax.Precision.HIGHEST)


def shards(
    prompt, norm_gain, gate_master, up_master, down_master, group_choice, inner_choice, route_weight
):
    experts = GROUPS * EPG
    scale = norm_gain[None, :, None]
    gate_cast = (gate_master * scale).astype(jnp.bfloat16)
    up_cast = (up_master * scale).astype(jnp.bfloat16)
    down_cast = down_master.astype(jnp.bfloat16)
    rows = gate_master.shape[1] // lax.axis_size("tp")
    values = prompt.astype(jnp.float32)
    normed = (values * lax.rsqrt(jnp.mean(values * values, axis=1, keepdims=True) + 1e-06)).astype(
        jnp.bfloat16
    )
    chosen = group_choice[:, None] * EPG + inner_choice
    member = (chosen[:, :, None] == jnp.arange(experts, dtype=jnp.int32)[None, None, :]).astype(
        jnp.float32
    )
    weight = jnp.sum(member * route_weight[:, :, None], axis=1)
    stacked = jnp.stack([gate_cast, up_cast, down_cast])
    widened = lax.all_to_all(stacked, "tp", split_axis=2, concat_axis=3, tiled=True)
    moved = lax.all_to_all(flatten_rows(widened), "fs", split_axis=2, concat_axis=1, tiled=True)
    served = restore_rows(lax.all_gather(moved, "tp", axis=1, tiled=True), rows)
    gate_local, up_local, down_local = (served[0], served[1], served[2])
    column_weight = route_columns(weight, gate_local.shape[1], experts)
    scaled = activations(normed, gate_local, up_local, column_weight)
    summed = lax.psum_scatter(
        lax.dot_general(
            down_local, scaled, (((1,), (1,)), ((), ())), preferred_element_type=jnp.float32
        ),
        "fs",
        scatter_dimension=0,
        tiled=True,
    )
    mixed = (summed * FF ** (-0.5)).T.astype(jnp.bfloat16)
    return (gate_local, up_local, down_local, mixed)


def remote(source, target, send, recv, device):
    return pltpu.make_async_remote_copy(
        src_ref=source,
        dst_ref=target,
        send_sem=send,
        recv_sem=recv,
        device_id=device,
        device_id_type=MESH,
    )


def block_order(groups):
    near = [2 * (i ^ (i >> 1)) + c for i in range(groups // 2) for c in range(2)]
    last = near[::-1]
    return near, [k for k in last if k % 2 == 1], [k for k in last if k % 2 == 0]


def matmul_nt(left, right):
    return lax.dot_general(left, right, (((1,), (1,)), ((), ())), preferred_element_type=jnp.float32)


def spread_body(
    gain_ref,
    gate_ref,
    up_ref,
    down_ref,
    prompt_ref,
    group_ref,
    inner_ref,
    route_ref,
    wide,
    down,
    scaled,
    got,
    raw,
    cast,
    gain,
    scale,
    prompt,
    normed,
    group,
    inner,
    route,
    column,
    part,
    load_sem,
    bulk_sem,
    small_sem,
    send_sem,
    zr,
    xr,
    yr,
    dr,
    pr,
    column_in,
):
    f, t = lax.axis_index("fs"), lax.axis_index("tp")
    tx, ty, td = jnp.bitwise_xor(t, 1), jnp.bitwise_xor(t, 2), jnp.bitwise_xor(t, 3)
    arrays, groups, per, rows, hidden = raw.shape
    parts, width = down.shape[:2]
    tokens = prompt.shape[0]
    half = rows // 2
    masters = (gate_ref, up_ref, down_ref)
    near, odds, evens = block_order(groups)
    order = [(w, k) for w in range(2) for k in near] + [(2, k) for k in odds + evens]
    base, split, lag = 2 * groups, 2 * groups + len(odds), groups // 2

    def peer(k):
        return jnp.bitwise_xor(f, k)

    def load(k):
        return pltpu.make_async_copy(gate_ref.at[peer(k)], raw.at[0, peer(k)], load_sem.at[k])

    def bulk(w):
        return pltpu.make_async_copy(masters[w], raw.at[w], bulk_sem.at[w - 1])

    small = [
        pltpu.make_async_copy(source, target, small_sem.at[i])
        for i, (source, target) in enumerate(
            (
                (gain_ref, gain),
                (prompt_ref, prompt),
                (group_ref, group),
                (inner_ref, inner),
                (route_ref, route),
            )
        )
    ]

    def block(w, origin, k, begin=0, count=rows):
        at = pl.ds(pl.multiple_of(peer(k) * rows + begin, count), count)
        return wide.at[w, origin, at] if w < 2 else down.at[origin, at]

    def z_copy(w, k):
        device = {"fs": peer(k), "tp": t}
        return remote(cast.at[w, k - 1], block(w, t, 0), send_sem.at[4], zr.at[w, k - 1], device)

    def z_arrival(w, k):
        device = {"fs": peer(k), "tp": t}
        return remote(cast.at[w, k - 1], block(w, t, k), send_sem.at[4], zr.at[w, k - 1], device)

    def x_copy(s, origin):
        one = block(order[s][0], origin, order[s][1])
        return remote(one, one, send_sem.at[s // base], xr.at[s % groups], {"fs": f, "tp": tx})

    def y_copy(s, origin):
        one = block(order[s][0], origin, order[s][1])
        return remote(one, one, send_sem.at[2 + s // base], yr.at[s % groups], {"fs": f, "tp": ty})

    def to_x(s):
        one = block(order[s][0], ty, order[s][1], half, half)
        return remote(one, one, send_sem.at[s // base], dr.at[s % groups], {"fs": f, "tp": tx})

    def to_y(s):
        one = block(order[s][0], tx, order[s][1], 0, half)
        return remote(one, one, send_sem.at[2 + s // base], dr.at[s % groups], {"fs": f, "tp": ty})

    def diagonal_wait(s):
        one = block(order[s][0], td, order[s][1])
        remote(one, one, send_sem.at[0], dr.at[s % groups], {"fs": f, "tp": tx}).wait_recv()

    def side_start(s):
        x_copy(s, t).start()
        y_copy(s, t).start()

    def side_half(s, begin):
        one = block(order[s][0], t, order[s][1], begin, half)
        remote(one, one, send_sem.at[s // base], xr.at[s % groups], {"fs": f, "tp": tx}).start()
        remote(one, one, send_sem.at[2 + s // base], yr.at[s % groups], {"fs": f, "tp": ty}).start()

    def forward(s):
        x_copy(s, tx).wait_recv()
        to_y(s).start()
        y_copy(s, ty).wait_recv()
        to_x(s).start()

    def put(w, k, target):
        for e in range(per):
            value = raw[w, peer(k), e]
            if w < 2:
                value = value * scale[...]
            target[:, e * hidden : (e + 1) * hidden] = value.astype(jnp.bfloat16)

    def put_all(w):
        bulk(w).wait()
        put(w, 0, block(w, t, 0))

        def one(k, carry):
            put(w, k, cast.at[w, k - 1])
            return carry

        lax.fori_loop(1, groups, one, 0)

    def normalise():
        small[1].wait()
        values = prompt[...].astype(jnp.float32)
        mean = jnp.mean(values * values, axis=1, keepdims=True)
        normed[...] = (values * lax.rsqrt(mean + 1e-06)).astype(jnp.bfloat16)

    def columns():
        for i in range(2, 5):
            small[i].wait()
        chosen = group[...] * EPG + inner[...]
        for e in range(per):
            weight = jnp.sum(jnp.where(chosen == f * per + e, route[...], 0.0), axis=0, keepdims=True)
            column[:, e * hidden : (e + 1) * hidden] = jnp.broadcast_to(weight, (hidden, tokens)).T

    def hidden_units(origin):
        step = 2 * hidden
        for n in range(per // 2):
            at = pl.ds(n * step, step)
            scaled[origin, :, at] = activations(
                normed[...], wide[0, origin, :, at], wide[1, origin, :, at], column[:, at]
            )

    def features(s):
        k = order[s][1]
        diagonal_wait(s)
        total = matmul_nt(scaled[0], block(2, 0, k)[...])
        for i in range(1, parts):
            total = total + matmul_nt(scaled[i], block(2, i, k)[...])
        part[s - base] = total.astype(jnp.bfloat16)
        device = {"fs": peer(k), "tp": t}
        remote(part.at[s - base], got.at[k - 1], send_sem.at[5], pr, device).start()

    small[0].start()
    load(0).start()
    barrier = pltpu.get_barrier_semaphore()

    def greet(chosen):
        for k in chosen:
            device = {"fs": peer(k), "tp": t}
            pl.semaphore_signal(barrier, inc=1, device_id=device, device_id_type=MESH)

    @pl.when(f % 2 == 0)
    def _():
        greet([1] + list(range(2, groups, 2)))

    @pl.when(f % 2 == 1)
    def _():
        greet(range(1, groups, 2))

    for other in (tx, ty):
        pl.semaphore_signal(barrier, inc=1, device_id={"fs": f, "tp": other}, device_id_type=MESH)
    small[0].wait()
    scale[...] = jnp.broadcast_to(gain[...], (hidden, rows)).T
    load(0).wait()
    put(0, 0, block(0, t, 0))
    for k in near[1:]:
        load(k).start()
    for w in (1, 2):
        bulk(w).start()
    for copy in small[1:]:
        copy.start()
    pl.semaphore_wait(barrier, 3 + (groups - 2) * (1 - f % 2))
    side_start(0)
    load(near[1]).wait()
    put(0, near[1], cast.at[0, near[1] - 1])

    @pl.when(f % 2 == 0)
    def _():
        pl.semaphore_signal(column_in, inc=1, device_id={"fs": peer(1), "tp": t}, device_id_type=MESH)

    @pl.when(f % 2 == 1)
    def _():
        pl.semaphore_wait(column_in, 1)

    for before, k in zip(near[1:], near[2:]):
        load(k).wait()
        put(0, k, cast.at[0, k - 1])
        z_copy(0, before).start()
    z_copy(0, near[-1]).start()

    near_sends = [(lag, 1, k) for k in near[1:4]] + [(groups + 5, 2, k) for k in near[1:4]]
    far = {1: near[4:], 2: [k for k in odds + evens if k >= 4]}
    inner_sends = [(lag + 2 + i // 2, 1, k) for i, k in enumerate(far[1])]
    inner_sends += [(groups + 4, 2, k) for k in far[2]]
    outer_sends = [(groups + 1, 1, k) for k in far[1]] + [(groups + 7, 2, k) for k in far[2]]
    outer = (f // 2 == 0) | (f // 2 == groups // 2 - 1)

    def send_at(s, chosen):
        for at, array, one in chosen:
            if at == s:
                z_copy(array, one).start()

    def step(s):
        w, k = order[s]
        if s > 0:
            if k > 0:
                z_arrival(w, k).wait_recv()
            if s == split:
                side_half(s, 0)
                forward(s - 1)
                side_half(s, half)
            else:
                side_start(s)
            if s == split + 1:
                features(s - 2)
            if s != split:
                forward(s - 1)
        send_at(s, near_sends)
        if any(at == s for at, _, _ in inner_sends):
            pl.when(jnp.logical_not(outer))(lambda: send_at(s, inner_sends))
        if any(at == s for at, _, _ in outer_sends):
            pl.when(outer)(lambda: send_at(s, outer_sends))
        if s < 2:
            put_all(s + 1)
        if s == groups:
            normalise()
            columns()
        if 3 <= s < base + 2:
            diagonal_wait(s - 3)
        if s == base:
            hidden_units(t)
        if s == base + 1:
            hidden_units(tx)
            hidden_units(ty)
        if s == base + 2:
            diagonal_wait(base - 1)
            hidden_units(td)
        if s >= base + 2 and s != split + 1:
            features(s - 2)

    def drain(end):
        forward(end - 1)
        features(end - 2)
        if order[end - 1][1] > 0:
            features(end - 1)
        else:
            diagonal_wait(end - 1)
        count = end - base
        sums = min(count, groups - 1)
        first = wide.at[:, pl.ds(0, parts - 1), pl.ds(0, width // 2)]
        second = down.at[pl.ds(0, parts - 1), pl.ds(0, count * half)]
        for i, whole in enumerate((first, second, first, second, cast, part.at[pl.ds(0, sums)])):
            remote(whole, whole, send_sem.at[i], pr, {"fs": f, "tp": tx}).wait_send()
        whole = got.at[pl.ds(0, sums)]
        remote(whole, whole, send_sem.at[5], pr, {"fs": f, "tp": tx}).wait_recv()

    for s in range(split):
        step(s)

    @pl.when(f % 2 == 1)
    def _():
        for k in evens[:-1]:
            z_arrival(2, k).wait_recv()
        drain(split)

    @pl.when(f % 2 == 0)
    def _():
        for s in range(split, len(order)):
            step(s)
        drain(len(order))


def spread(prompt, norm_gain, gate_master, up_master, down_master, group_choice, inner_choice, route_weight):
    groups, parts = lax.axis_size("fs"), lax.axis_size("tp")
    experts, rows, hidden = gate_master.shape
    per = experts // groups
    tokens, width = prompt.shape
    arrays = 3
    views = [one.reshape(groups, per, rows, hidden) for one in (gate_master, up_master, down_master)]
    dma = pltpu.SemaphoreType.DMA
    return pl.pallas_call(
        spread_body,
        in_specs=[pl.BlockSpec(memory_space=pltpu.HBM)] * 8,
        out_specs=[pl.BlockSpec(memory_space=pltpu.VMEM)] * 4,
        out_shape=[
            pltpu.VMEM((2, parts, width, per * hidden), jnp.bfloat16),
            pltpu.VMEM((parts, width, per * hidden), jnp.bfloat16),
            pltpu.VMEM((parts, tokens, per * hidden), jnp.bfloat16),
            pltpu.VMEM((groups - 1, tokens, rows), jnp.bfloat16),
        ],
        scratch_shapes=[
            pltpu.VMEM((arrays, groups, per, rows, hidden), jnp.float32),
            pltpu.VMEM((arrays, groups - 1, rows, per * hidden), jnp.bfloat16),
            pltpu.VMEM((1, rows), jnp.float32),
            pltpu.VMEM((rows, hidden), jnp.float32),
            pltpu.VMEM((tokens, width), jnp.bfloat16),
            pltpu.VMEM((tokens, width), jnp.bfloat16),
            pltpu.VMEM((1, tokens), jnp.int32),
            pltpu.VMEM((2, tokens), jnp.int32),
            pltpu.VMEM((2, tokens), jnp.float32),
            pltpu.VMEM((tokens, per * hidden), jnp.float32),
            pltpu.VMEM((groups - 1, tokens, rows), jnp.bfloat16),
            dma((groups,)),
            dma((2,)),
            dma((5,)),
            dma((6,)),
            dma((arrays, groups - 1)),
            dma((groups,)),
            dma((groups,)),
            dma((groups,)),
            dma,
            pltpu.SemaphoreType.REGULAR,
        ],
        compiler_params=pltpu.CompilerParams(
            collective_id=0, has_side_effects=True, vmem_limit_bytes=32 * 1024 * 1024
        ),
        name="spread",
    )(
        norm_gain.reshape(1, rows),
        *views,
        prompt,
        group_choice.reshape(1, tokens),
        inner_choice.T,
        route_weight.T,
    )


def store_body(wide, down, gate_ref, up_ref, down_ref, token_ref, sem):
    parts, width, hold = down.shape
    hidden = FF // parts
    groups, per = lax.axis_size("fs"), hold // hidden
    rows = width // groups
    f = lax.axis_index("fs")
    _, odds, evens = block_order(groups)

    def put(k):
        at = pl.ds(pl.multiple_of(jnp.bitwise_xor(f, k) * rows, rows), rows)
        for i in range(parts):
            for e in range(per):
                pltpu.make_async_copy(
                    down.at[i, at, pl.ds(e * hidden, hidden)],
                    down_ref.at[at, pl.ds(e * FF + i * hidden, hidden)],
                    sem.at[2],
                ).start()

    def wait(count):
        done = down_ref.at[pl.ds(0, count * rows)]
        pltpu.make_async_copy(done, done, sem.at[2]).wait()

    outs = (gate_ref, up_ref)
    for w, out in enumerate(outs):
        for i in range(parts):
            for e in range(per):
                pltpu.make_async_copy(
                    wide.at[w, i, :, pl.ds(e * hidden, hidden)],
                    out.at[:, pl.ds(e * FF + i * hidden, hidden)],
                    sem.at[w],
                ).start()
    for k in odds:
        put(k)

    @pl.when(f % 2 == 0)
    def _():
        for k in evens:
            put(k)
        wait(groups)

    @pl.when(f % 2 == 1)
    def _():
        wait(len(odds))

    for w, out in enumerate(outs):
        pltpu.make_async_copy(out, out, sem.at[w]).wait()


def hold_in_vmem(*arrays):
    return [pltpu.with_memory_space_constraint(one, pltpu.VMEM) for one in arrays]


def store(wide, down):
    parts, width, hold = down.shape
    out = pltpu.HBM((width, parts * hold), down.dtype)
    vmem, hbm = pl.BlockSpec(memory_space=pltpu.VMEM), pl.BlockSpec(memory_space=pltpu.HBM)
    return pl.pallas_call(
        store_body,
        in_specs=[vmem, vmem],
        out_specs=[hbm, hbm, hbm, hbm],
        out_shape=[out, out, out, pltpu.HBM((8, 128), jnp.float32)],
        scratch_shapes=[pltpu.SemaphoreType.DMA((3,))],
        compiler_params=pltpu.CompilerParams(vmem_limit_bytes=4 * 1024 * 1024),
        name="store",
    )(*hold_in_vmem(wide, down))


def finish_body(down, scaled, got, token_ref, late, got_late, mine, part, send_sem, xr, yr, dr, pr):
    f, t = lax.axis_index("fs"), lax.axis_index("tp")
    tx, ty = jnp.bitwise_xor(t, 1), jnp.bitwise_xor(t, 2)
    parts = down.shape[0]
    rows = late.shape[2]
    half, quarter = rows // 2, rows // 4
    _, odds, evens = block_order(lax.axis_size("fs"))
    count = len(evens)

    def own(i, begin=0, size=rows):
        first = jnp.bitwise_xor(f, evens[i]) * rows + begin
        return down.at[t, pl.ds(pl.multiple_of(first, size), size)]

    pieces = [(i, c * half, half) for i in range(count) for c in range(2)]
    pieces[-1:] = [(count - 1, half, quarter), (count - 1, half + quarter, quarter)]

    def landed(j, q, which=None):
        i, begin, size = pieces[q]
        if which is not None:
            size = size // 2
            begin = begin + which * size
        return late.at[j, i, pl.ds(begin, size)]

    def x_copy(q):
        source = own(*pieces[q])
        return remote(source, landed(0, q), send_sem.at[0], xr.at[q], {"fs": f, "tp": tx})

    def y_copy(q):
        source = own(*pieces[q])
        return remote(source, landed(1, q), send_sem.at[1], yr.at[q], {"fs": f, "tp": ty})

    def to_y(q):
        source, target = landed(0, q, 0), landed(2, q, 0)
        return remote(source, target, send_sem.at[1], dr.at[pieces[q][0]], {"fs": f, "tp": ty})

    def to_x(q):
        source, target = landed(1, q, 1), landed(2, q, 1)
        return remote(source, target, send_sem.at[0], dr.at[pieces[q][0]], {"fs": f, "tp": tx})

    def side_start(q):
        x_copy(q).start()
        y_copy(q).start()

    def forward(q):
        x_copy(q).wait_recv()
        to_y(q).start()
        y_copy(q).wait_recv()
        to_x(q).start()

    def straight(i):
        total = matmul_nt(scaled[t], own(i)[...])
        for j in (1, 2):
            total = total + matmul_nt(scaled[jnp.bitwise_xor(t, j)], late[j - 1, i])
        return total

    def diagonal_wait(i):
        one = late.at[2, i]
        remote(one, one, send_sem.at[0], dr.at[i], {"fs": f, "tp": tx}).wait_recv()

    def features(i):
        mine[...] = straight(i)
        diagonal_wait(i)
        total = mine[...] + matmul_nt(scaled[jnp.bitwise_xor(t, 3)], late[2, i])
        part[i] = total.astype(jnp.bfloat16)
        device = {"fs": jnp.bitwise_xor(f, evens[i]), "tp": t}
        remote(part.at[i], got_late.at[i], send_sem.at[2], pr, device).start()

    def collected(total, chosen):
        for k in chosen:
            total = total + got[k - 1].astype(jnp.float32)
        return total

    def run():
        total, sent = len(pieces), 0
        for q in range(total):
            goal = 4 if q == 0 else 5 + q // 2
            if q >= 2 * count - 2:
                goal = total
            while sent < min(goal, total):
                side_start(sent)
                sent += 1
            if q >= 4 and q % 2 == 0 and q < 2 * count - 1:
                features(q // 2 - 2)
            forward(q)
            if q == 2 * count - 2:
                features(count - 2)
        mine[...] = collected(straight(count - 1), odds)
        diagonal_wait(count - 1)
        sides = late.at[:, :, pl.ds(0, half)]
        for i, whole in enumerate((sides, sides, part)):
            remote(whole, whole, send_sem.at[i], pr, {"fs": f, "tp": tx}).wait_send()
        remote(got_late, got_late, send_sem.at[2], pr, {"fs": f, "tp": tx}).wait_recv()

    @pl.when(f % 2 == 1)
    def _():
        barrier = pltpu.get_barrier_semaphore()
        others = [{"fs": jnp.bitwise_xor(f, k), "tp": t} for k in evens[:-1]]
        others += [{"fs": f, "tp": tx}, {"fs": f, "tp": ty}]
        for other in others:
            pl.semaphore_signal(barrier, inc=1, device_id=other, device_id_type=MESH)
        pl.semaphore_wait(barrier, len(others))
        run()

    @pl.when(f % 2 == 0)
    def _():
        at = pl.ds(pl.multiple_of(f * rows, rows), rows)
        total = matmul_nt(scaled[0], down[0, at, :])
        for i in range(1, parts):
            total = total + matmul_nt(scaled[i], down[i, at, :])
        mine[...] = collected(total, odds + evens[:-1])


def finish(down, scaled, got, token, groups):
    parts, width, hold = down.shape
    tokens, rows, count = scaled.shape[1], width // groups, groups // 2
    vmem, hbm = pl.BlockSpec(memory_space=pltpu.VMEM), pl.BlockSpec(memory_space=pltpu.HBM)
    dma = pltpu.SemaphoreType.DMA
    return pl.pallas_call(
        finish_body,
        in_specs=[vmem, vmem, vmem, hbm],
        out_specs=[vmem, vmem, vmem],
        out_shape=[
            pltpu.VMEM((parts - 1, count, rows, hold), down.dtype),
            pltpu.VMEM((count - 1, tokens, rows), jnp.bfloat16),
            pltpu.VMEM((tokens, rows), jnp.float32),
        ],
        scratch_shapes=[
            pltpu.VMEM((count - 1, tokens, rows), jnp.bfloat16),
            dma((3,)),
            dma((2 * count + 1,)),
            dma((2 * count + 1,)),
            dma((count,)),
            dma,
        ],
        compiler_params=pltpu.CompilerParams(
            collective_id=1, has_side_effects=True, vmem_limit_bytes=4 * 1024 * 1024
        ),
        name="finish",
    )(*hold_in_vmem(down, scaled, got), pltpu.with_memory_space_constraint(token, pltpu.HBM))


def serve_body(down, late, scaled, got_late, mine, down_in, down_ref, mixed_ref, mixed, sem):
    parts, width, hold = down.shape
    hidden, rows = FF // parts, late.shape[2]
    f, t = lax.axis_index("fs"), lax.axis_index("tp")
    _, _, evens = block_order(width // rows)
    count = len(evens)

    def put(i):
        at = pl.ds(pl.multiple_of(jnp.bitwise_xor(f, evens[i]) * rows, rows), rows)
        for j in range(parts):
            origin = jnp.bitwise_xor(t, j)
            source = late.at[j - 1, i] if j > 0 else down.at[t, at]
            for e in range(hold // hidden):
                begin = pl.multiple_of(e * FF + origin * hidden, hidden)
                pltpu.make_async_copy(
                    source.at[:, pl.ds(e * hidden, hidden)], down_ref.at[at, pl.ds(begin, hidden)], sem.at[0]
                ).start()

    def finish_mixed(total):
        mixed[...] = (total * FF ** (-0.5)).astype(jnp.bfloat16)
        final = pltpu.make_async_copy(mixed, mixed_ref, sem.at[1])
        final.start()
        return final

    @pl.when(f % 2 == 1)
    def _():
        for i in range(count):
            put(i)
        total = mine[...] + matmul_nt(scaled[jnp.bitwise_xor(t, 3)], late[2, count - 1])
        for i in range(count - 1):
            total = total + got_late[i].astype(jnp.float32)
        final = finish_mixed(total)
        done = down_ref.at[pl.ds(0, count * rows)]
        pltpu.make_async_copy(done, done, sem.at[0]).wait()
        final.wait()

    @pl.when(f % 2 == 0)
    def _():
        finish_mixed(mine[...]).wait()


def serve(down, late, scaled, got_late, mine, down_out):
    tokens, rows = mine.shape
    vmem, hbm = pl.BlockSpec(memory_space=pltpu.VMEM), pl.BlockSpec(memory_space=pltpu.HBM)
    return pl.pallas_call(
        serve_body,
        in_specs=[vmem] * 5 + [hbm],
        out_specs=[hbm, hbm],
        out_shape=[pltpu.HBM(down_out.shape, down_out.dtype), pltpu.HBM((tokens, rows), jnp.bfloat16)],
        input_output_aliases={5: 0},
        scratch_shapes=[pltpu.VMEM((tokens, rows), jnp.bfloat16), pltpu.SemaphoreType.DMA((2,))],
        compiler_params=pltpu.CompilerParams(vmem_limit_bytes=4 * 1024 * 1024),
        name="serve",
    )(*hold_in_vmem(down, late, scaled, got_late, mine), pltpu.with_memory_space_constraint(down_out, pltpu.HBM))


def direct_shards(
    prompt, norm_gain, gate_master, up_master, down_master, group_choice, inner_choice, route_weight
):
    groups = lax.axis_size("fs")
    wide, down, scaled, got = spread(
        prompt, norm_gain, gate_master, up_master, down_master, group_choice, inner_choice, route_weight
    )
    gate_local, up_local, down_some, token = store(wide, down)
    late, got_late, mine = finish(down, scaled, got, token, groups)
    down_local, mixed = serve(down, late, scaled, got_late, mine, down_some)
    return (gate_local, up_local, down_local, mixed)


def fits_direct(mesh):
    groups, parts = mesh.shape["fs"], mesh.shape["tp"]
    whole_experts = (GROUPS * EPG) % groups == 0 and (GROUPS * EPG // groups) % 2 == 0
    return parts == 4 and groups >= 4 and groups & (groups - 1) == 0 and whole_experts and FF // parts % 128 == 0


def solution(mesh):
    in_specs = (
        P("tp", None),
        P("fs"),
        P(None, "fs", "tp"),
        P(None, "fs", "tp"),
        P(None, "fs", "tp"),
        P("tp"),
        P("tp", None),
        P("tp", None),
    )
    out_specs = (P(None, "fs"), P(None, "fs"), P(None, "fs"), P("tp", "fs"))
    body = direct_shards if fits_direct(mesh) else shards
    return jax.shard_map(body, mesh=mesh, in_specs=in_specs, out_specs=out_specs, check_vma=False)
```
